256 devices in a mesh: sp: 16 (over y, x), tp: 16 (over z, core).
Axes of the slice: x: 4, y: 4, z: 8, core: 2. Of those that a mesh axis runs over, the one named last changes fastest.
Arguments:
- latent: bfloat16 [8192, 4096], P(('sp', 'tp')), may hold values from -6 to 6
- context: bfloat16 [512, 4096], P('sp'), may hold values from -6 to 6
- condition: float32 [4096], replicated, may hold values from -6 to 6
- context_condition: float32 [4096], replicated, may hold values from -6 to 6
- modulation: bfloat16 [3, 4096, 4096], P(None, 'sp', 'tp'), may hold values from -0.09375 to 0.09375
- query_weight: bfloat16 [4096, 4096], P(None, 'tp'), as said below
- key_weight: bfloat16 [4096, 4096], P(None, 'tp'), as said below
- value_weight: bfloat16 [4096, 4096], P(None, 'tp'), may hold values from -0.09375 to 0.09375
- lambdas: float32 [16], P('tp'), may hold values from 0.3 to 0.8
- context_lift: float32 [16], P('tp'), may hold values from 1.5 to 3
- head_gain: float32 [256], replicated, may hold values from 0.1 to 1.9
- output_weight: bfloat16 [4096, 4096], P('tp'), may hold values from -0.09375 to 0.09375
Outputs:
- result: bfloat16 [8192, 4096], P(('sp', 'tp'))
The draws below stay inside these ranges and needn't reach their ends.
Inputs may be any that keep to these rules, and one draw needn't show every extreme that they name: `query_weight`: entries lie within 200 / sqrt(4096) in magnitude. `key_weight`: entries lie within 6 / sqrt(4096) in magnitude.
All inputs are finite; a program needn't handle non-finite values.
Results may differ from the reference program's by a relative error of at most 0.025.
Values may be sent and summed in bfloat16 or wider, within the bound.
A program may use at most 64 MiB of HBM per device.

```python
import math
import jax
import jax.numpy as jnp
from jax import lax

D = 4096
HEADS = 16
HEAD_DIM = 256
GRID_W = 64
CTX = 512
SEQ = 8192


def common_keys(key):
    gaussian = jax.random.normal(jax.random.fold_in(key, 101), (D, HEADS * HEAD_DIM), jnp.float32)
    return jnp.clip(gaussian, -6.0, 6.0) * D ** (-0.5)


def draw_key_weight(key, part):
    return common_keys(key).astype(jnp.bfloat16)


def draw_query_weight(key, part):
    gaussian = jax.random.normal(jax.random.fold_in(key, 202), (D, HEADS * HEAD_DIM), jnp.float32)
    independent = jnp.clip(gaussian, -6.0, 6.0) * D ** (-0.5)
    return independent.astype(jnp.bfloat16)


def steps_of(rng, extent, shards, low, high):
    gain, own = 1.0, jax.random.fold_in(rng, 6)
    for dim, shards_of in shards:
        heights = jnp.exp(jax.random.uniform(jax.random.fold_in(own, dim), (shards_of,), jnp.float32, low / len(shards), high / len(shards)))
        gain = gain * jnp.repeat(heights, extent[dim] // shards_of).reshape([-1 if axis == dim else 1 for axis in range(len(extent))])
    return gain


def scatter_about(own_key, extent, scale, reach, cuts=(), kind=jnp.bfloat16):
    factor_of = steps_of(own_key, extent, cuts, -0.22, 0.18) if cuts else 1.0
    values = jax.random.normal(own_key, extent, jnp.float32) * scale * factor_of
    return jnp.minimum(jnp.maximum(values, -reach), reach).astype(kind)


def setup_inputs(seed: int = 0) -> dict:
    keys = jax.random.split(jax.random.key(seed), 13)
    latent = scatter_about(keys[0], (SEQ, D), 1.0, 6.0, ((0, 256),))
    context = scatter_about(keys[1], (CTX, D), 1.0, 6.0, ((0, 16),))
    condition = scatter_about(keys[2], (D,), 1.0, 6.0, (), jnp.float32)
    context_condition = scatter_about(keys[3], (D,), 1.0, 6.0, (), jnp.float32)
    modulation = scatter_about(keys[4], (3, D, D), D ** -0.5, 0.09375, ((1, 16), (2, 16)))
    query_weight = draw_query_weight(jax.random.fold_in(keys[12], 71), 0)
    key_weight = draw_key_weight(jax.random.fold_in(keys[12], 71), 0)
    value_weight = scatter_about(keys[7], (D, HEADS * HEAD_DIM), D ** -0.5, 0.09375, ((1, 16),))
    lambdas = jnp.clip(0.3 + 0.5 * jax.random.uniform(keys[8], (HEADS,), jnp.float32) ** steps_of(keys[8], (HEADS,), ((0, 16),), -0.2, 0.2), 0.3, 0.8)
    context_lift = jnp.clip(1.5 + 1.5 * jax.random.uniform(keys[9], (HEADS,), jnp.float32) ** steps_of(keys[9], (HEADS,), ((0, 16),), -0.2, 0.2), 1.5, 3.0)
    head_gain = jnp.clip(1.0 + 0.18 * jax.random.normal(keys[10], (HEAD_DIM,), jnp.float32), 0.1, 1.9)
    output_weight = scatter_about(keys[11], (HEADS * HEAD_DIM, D), (HEADS * HEAD_DIM) ** -0.5, 0.09375, ((0, 16),))
    return {"latent": latent, "context": context, "condition": condition, "context_condition": context_condition, "modulation": modulation, "query_weight": query_weight, "key_weight": key_weight, "value_weight": value_weight, "lambdas": lambdas, "context_lift": context_lift, "head_gain": head_gain, "output_weight": output_weight}


ROPE_BASE = 10000.0
EPSILON = 1e-05

def modulate(tokens_in, offset, scaling):
    values = tokens_in.astype(jnp.float32)
    center = lax.optimization_barrier(jnp.mean(values, axis=-1, keepdims=True))
    spread = lax.optimization_barrier(jnp.mean(jnp.square(values - center), axis=-1, keepdims=True))
    normed = (values - center) * lax.rsqrt(spread + EPSILON)
    return (normed * (1.0 + scaling) + offset).astype(jnp.bfloat16)

def rotate(tensor, places):
    number, head_count, head_width = tensor.shape
    quarter = head_width // 4
    eighth = head_width // 8
    inverse = ROPE_BASE ** (-jnp.arange(eighth, dtype=jnp.float32) / eighth)
    grid_row = (places // GRID_W).astype(jnp.float32)
    grid_col = (places % GRID_W).astype(jnp.float32)
    angles = jnp.stack([grid_row[:, None] * inverse, grid_col[:, None] * inverse], axis=1)
    cosine = jnp.cos(angles)[:, None, None, :, :]
    sine_table = jnp.sin(angles)[:, None, None, :, :]
    pieces = tensor.reshape(number, head_count, 2, 2, quarter)
    first_half = pieces[..., :eighth]
    second = pieces[..., eighth:]
    turned = jnp.concatenate([first_half * cosine - second * sine_table, second * cosine + first_half * sine_table], axis=-1)
    return turned.reshape(number, head_count, head_width)

def reference(latent, context, condition, context_condition, modulation, query_weight, key_weight, value_weight, lambdas, context_lift, head_gain, output_weight):
    silu_pair = jax.nn.silu(jnp.stack([condition, context_condition])).astype(jnp.bfloat16)
    mod_vectors = jnp.einsum('cd,rde->cre', silu_pair.astype(jnp.float32), modulation.astype(jnp.float32))
    normed = modulate(latent, mod_vectors[0, 0], mod_vectors[0, 1])
    normed_context = modulate(context, mod_vectors[1, 0], mod_vectors[1, 1])
    seq_len = latent.shape[0]
    half_width = HEAD_DIM // 2
    scale_factor = half_width ** (-0.5)
    query_raw = jnp.dot(normed, query_weight, preferred_element_type=jnp.float32).astype(jnp.bfloat16)
    key_raw = jnp.dot(normed, key_weight, preferred_element_type=jnp.float32).astype(jnp.bfloat16)
    latent_values = jnp.dot(normed, value_weight, preferred_element_type=jnp.float32).astype(jnp.bfloat16)
    context_keys = jnp.dot(normed_context, key_weight, preferred_element_type=jnp.float32).astype(jnp.bfloat16)
    context_values = jnp.dot(normed_context, value_weight, preferred_element_type=jnp.float32).astype(jnp.bfloat16)
    places = jnp.arange(seq_len, dtype=jnp.int32)
    queries = rotate(query_raw.astype(jnp.float32).reshape(seq_len, HEADS, HEAD_DIM), places).astype(jnp.bfloat16)
    latent_keys = rotate(key_raw.astype(jnp.float32).reshape(seq_len, HEADS, HEAD_DIM), places).astype(jnp.bfloat16)
    all_keys = jnp.concatenate([context_keys.reshape(CTX, HEADS, HEAD_DIM), latent_keys], axis=0)
    all_values = jnp.concatenate([context_values.reshape(CTX, HEADS, HEAD_DIM), latent_values.reshape(seq_len, HEADS, HEAD_DIM)], axis=0)
    key_total = CTX + seq_len
    block_len = math.gcd(seq_len, 1024)

    def one_head(inputs):
        head_queries, head_keys, head_values, head_lambda, head_lift = inputs
        lift_row = jnp.where(jnp.arange(key_total) < CTX, head_lift, 0.0)

        def one_block(block_queries):
            outputs = []
            for map_index in range(2):
                low_col = map_index * half_width
                scores = jnp.dot(block_queries[:, low_col:low_col + half_width], head_keys[:, low_col:low_col + half_width].T, preferred_element_type=jnp.float32) * scale_factor + lift_row
                row_peak = lax.optimization_barrier(jnp.max(scores, axis=1, keepdims=True))
                weights = jnp.exp(scores - row_peak)
                row_sums = lax.optimization_barrier(jnp.sum(weights, axis=1, keepdims=True))
                outputs.append(jnp.dot(weights.astype(jnp.bfloat16), head_values, preferred_element_type=jnp.float32) / row_sums)
            difference = outputs[0] - head_lambda * outputs[1]
            scaled = difference * lax.rsqrt(lax.optimization_barrier(jnp.mean(jnp.square(difference), axis=1, keepdims=True)) + EPSILON) * head_gain
            return scaled.astype(jnp.bfloat16)
        blocks = head_queries.reshape(seq_len // block_len, block_len, HEAD_DIM)
        return lax.map(one_block, blocks).reshape(seq_len, HEAD_DIM)
    heads_out = lax.map(one_head, (queries.transpose(1, 0, 2), all_keys.transpose(1, 0, 2), all_values.transpose(1, 0, 2), lambdas, context_lift))
    attended = heads_out.transpose(1, 0, 2).reshape(seq_len, HEADS * HEAD_DIM)
    mixture = jnp.dot(attended, output_weight, preferred_element_type=jnp.float32)
    return (latent.astype(jnp.float32) + mod_vectors[0, 2] * mixture).astype(jnp.bfloat16)
```

```python
import functools
import math

import jax
import jax.numpy as jnp
import numpy as np
from jax import lax
from jax.experimental import pallas as pl
from jax.experimental.pallas import tpu as pltpu
from jax.sharding import Mesh
from jax.sharding import PartitionSpec as P

MESH = pl.DeviceIdType.MESH
F32 = jnp.float32
BF16 = jnp.bfloat16

WIDTH = 4096
GRID_W = 64
ROPE_BASE = 10000.0
EPSILON = 1e-05
HEAD = 256
PART = 128
LOG2E = math.log2(math.e)
SCALE2 = PART ** (-0.5) * LOG2E
ROWS = 512
OWN = 32
CTX = 32
MEMBERS = 4
LAT_KEYS = MEMBERS * ROWS
KEYS = LAT_KEYS + MEMBERS * CTX
TILE = 256
OFFSET = (0, -1, 1, -2, 2, -3, 3, 4)
PASSES = ((0,), (1, 2), (3, 4), (5, 6), (7,))


def rope_tables():
    quarter = PART // 2
    eighth = PART // 4
    inverse = np.float32(ROPE_BASE) ** (-np.arange(eighth, dtype=np.float32) / np.float32(eighth))
    inverse = inverse.astype(np.float32)
    sign = np.concatenate([-np.ones(eighth), np.ones(eighth)]).astype(np.float32)

    def pair(count):
        angles = np.arange(count, dtype=np.float32)[:, None] * np.concatenate([inverse, inverse])
        angles = angles.astype(np.float32).astype(np.float64)
        return np.cos(angles).astype(np.float32), (np.sin(angles) * sign).astype(np.float32)

    row_cos, row_sin = pair(8192 // GRID_W)
    col_cos, col_sin = pair(GRID_W)
    none = np.zeros_like(row_cos)
    row_cos, row_sin = (np.concatenate([t, none], axis=1) for t in (row_cos, row_sin))
    none = np.zeros_like(col_cos)
    col_cos, col_sin = (np.concatenate([none, t], axis=1) for t in (col_cos, col_sin))
    half = GRID_W // 2
    both = [np.stack([t, np.concatenate([t[half:], t[:half]])]) for t in (col_cos, col_sin)]
    return row_cos, row_sin, both[0], both[1]


def body(
    latent,
    context,
    condition,
    context_condition,
    modulation,
    query_weight,
    key_weight,
    value_weight,
    lambdas,
    context_lift,
    head_gain,
    output_weight,
    row_cos,
    row_sin,
    col_cos,
    col_sin,
    result,
    gx,
    ctx,
    modw,
    weights,
    xn,
    mod_y,
    mod_x,
    mod_all,
    raw,
    qs,
    kv,
    outs,
    outs_in,
    stats,
    stats_in,
    att,
    att_in,
    wout,
    part,
    sum_out,
    sum_in,
    load_sem,
    xs,
    xr,
    ps,
    pr,
    ms,
    mr,
    zs,
    zr,
    fs,
    fr,
    qsem_s,
    qsem_r,
    ksem_s,
    ksem_r,
    csem_s,
    csem_r,
    osem_s,
    osem_r,
    tsem_s,
    tsem_r,
    asem,
    wsem,
    rs,
    rr,
):
    y, x, z, c = (lax.axis_index(a) for a in ("y", "x", "z", "c"))
    sp = y * 4 + x
    waits = []

    def remote(src, dst, send, recv, to):
        return pltpu.make_async_remote_copy(
            src_ref=src, dst_ref=dst, send_sem=send, recv_sem=recv, device_id=to, device_id_type=MESH
        )

    def go(copy):
        copy.start()
        waits.append(copy)

    partner = {"c": 1 - c}

    def on_y(d):
        return {"y": lax.rem(y + d, 4)}

    def on_x(d):
        return {"x": lax.rem(x + d, 4)}

    def on_z(d):
        return {"z": lax.rem(z + d + 8, 8)}

    def on_queries(d):
        return {"y": lax.rem(y + d * c, 4), "x": lax.rem(x + d * (1 - c), 4)}

    def on_keys(d):
        return {"y": lax.rem(y + d * (1 - c), 4), "x": lax.rem(x + d * c, 4)}

    loads = [
        pltpu.make_async_copy(latent, gx.at[0, pl.ds(0, OWN)], load_sem.at[0]),
        pltpu.make_async_copy(modulation, modw, load_sem.at[1]),
        pltpu.make_async_copy(context, ctx, load_sem.at[2]),
        pltpu.make_async_copy(query_weight, weights.at[0], load_sem.at[3]),
        pltpu.make_async_copy(key_weight, weights.at[1], load_sem.at[4]),
        pltpu.make_async_copy(value_weight, weights.at[2], load_sem.at[5]),
        pltpu.make_async_copy(output_weight, wout.at[0], load_sem.at[6]),
    ]
    for load in loads:
        load.start()

    barrier = pltpu.get_barrier_semaphore()
    peers = [on_y(d) for d in (1, 2, 3)] + [on_x(d) for d in (1, 2, 3)]
    peers += [on_z(d) for d in range(1, 8)] + [partner]
    for peer in peers:
        pl.semaphore_signal(barrier, inc=1, device_id=peer, device_id_type=MESH)
    pl.semaphore_wait(barrier, len(peers))

    def ring_slot(way, k):
        return 0 if k == 0 else 7 if k == 4 else 2 * k - 1 if way == 0 else 2 * k

    def ring_copy(way, k, h):
        rows = pl.ds(16 * h, 16)
        return remote(
            gx.at[ring_slot(way, k - 1), rows],
            gx.at[ring_slot(way, k), rows],
            xs.at[way, k - 1, h],
            xr.at[way, k - 1, h],
            on_z(1 if way == 0 else -1),
        )

    def across(slot, h):
        return remote(
            gx.at[slot, pl.ds(16 * h, 16)],
            gx.at[slot, pl.ds(OWN + 16 * h, 16)],
            ps.at[slot, h],
            pr.at[slot, h],
            partner,
        )

    def relay(k, turn):
        for way in (0, 1):
            h = turn if way == 0 else 1 - turn
            if k == 4 and turn == 1:
                continue
            ring_copy(way, k, h).wait_recv()
            if k < 3 or (k == 3 and turn == 0):
                go(ring_copy(way, k + 1, h))
            go(across(ring_slot(way, k), h))

    loads[0].wait()
    for turn in (0, 1):
        for way in (0, 1):
            go(ring_copy(way, 1, turn if way == 0 else 1 - turn))
    for h in (0, 1):
        go(across(0, h))

    def silu_rows(ref):
        halves = [ref[pl.ds(2 * sp + i, 1), :] for i in (0, 1)]
        v = jnp.concatenate(halves, axis=1)
        return (v / (1.0 + jnp.exp(-v))).astype(BF16).astype(F32)

    own = silu_rows(condition)
    other = silu_rows(context_condition)
    at_row = lax.broadcasted_iota(jnp.int32, (16, 256), 0)
    loads[1].wait()
    partial = jnp.zeros((16, 256), F32)
    for r in range(3):
        lhs = jnp.where(at_row == 2 * r, own, jnp.where(at_row == 2 * r + 1, other, 0.0))
        partial += jnp.dot(lhs.astype(BF16), modw[r], preferred_element_type=F32)
    mod_y[0] = partial[:8]

    def mod_copy(buf, stage, d, to):
        return remote(buf.at[0], buf.at[4 - d], ms.at[stage, d], mr.at[stage, 4 - d], to)

    for d in (2, 1, 3):
        go(mod_copy(mod_y, 0, d, on_y(d)))
    for d in (2, 1, 3):
        mod_copy(mod_y, 0, d, on_y(d)).wait_recv()
    mod_x[0] = (mod_y[0] + mod_y[1]) + (mod_y[2] + mod_y[3])
    for d in (2, 1, 3):
        go(mod_copy(mod_x, 1, d, on_x(d)))
    for d in (2, 1, 3):
        mod_copy(mod_x, 1, d, on_x(d)).wait_recv()
    mod_all[z, c] = (mod_x[0] + mod_x[1]) + (mod_x[2] + mod_x[3])
    for d in (4, 3, 5, 2, 6, 1, 7):
        go(remote(mod_all.at[z, c], mod_all.at[z, c], zs.at[d], zr.at[8 - d], on_z(d)))
    go(remote(mod_all.at[z, c], mod_all.at[z, c], fs.at[0], fr.at[0], partner))
    relay(1, 0)
    relay(1, 1)
    for d in range(1, 8):
        there = lax.rem(z + d, 8)
        slab = mod_all.at[there, c]
        remote(slab, slab, zs.at[d], zr.at[d], on_z(d)).wait_recv()
        go(remote(slab, slab, fs.at[d], fr.at[d], partner))
    relay(2, 0)
    for d in range(8):
        slab = mod_all.at[lax.rem(z + d, 8), 1 - c]
        remote(slab, slab, fs.at[d], fr.at[d], partner).wait_recv()

    def normalize(src, dst_row, which, groups):
        def group(g, carry):
            v = src[pl.ds(pl.multiple_of(g * 16, 16), 16), :].astype(F32)
            center = jnp.mean(v, axis=-1, keepdims=True)
            v = v - center
            spread = jnp.mean(jnp.square(v), axis=-1, keepdims=True)
            inverse = lax.rsqrt(spread + EPSILON)
            for t in range(16):
                cols = slice(t * 256, (t + 1) * 256)
                offset = mod_all[t // 2, t % 2, which : which + 1, :]
                scaling = mod_all[t // 2, t % 2, 2 + which : 3 + which, :]
                done = (v[:, cols] * inverse) * (1.0 + scaling) + offset
                xn[pl.ds(pl.multiple_of(dst_row + g * 16, 16), 16), cols] = done.astype(BF16)
            return carry

        lax.fori_loop(0, groups, group, 0)

    lane = lax.broadcasted_iota(jnp.int32, (64, PART), 1)
    low = lax.rem(lane, 64) < 32

    def project(count):
        def one(g, carry):
            raw[g, pl.ds(0, count)] = jnp.dot(
                xn[pl.ds(0, count), :], weights[g], preferred_element_type=F32
            ).astype(BF16)
            return carry

        lax.fori_loop(0, 3, one, 0)

    def step(p):
        slots = PASSES[p]
        for i, slot in enumerate(slots):
            normalize(gx.at[slot], 64 * i, 0, 4)
        count = 64 * len(slots)
        if p == 0:
            loads[2].wait()
            normalize(ctx, 64, 1, 2)
            count += CTX
            for load in loads[3:6]:
                load.wait()
        project(count)
        for i, slot in enumerate(slots):
            line = sp * 8 + lax.rem(z + OFFSET[slot] + 8, 8)
            cosine = col_cos[c] + row_cos[pl.ds(line, 1), :]
            sine = col_sin[c] + row_sin[pl.ds(line, 1), :]
            base = 64 * slot
            for g in (0, 1):
                for m in (0, 1):
                    cols = slice(m * PART, (m + 1) * PART)
                    a = raw[g, 64 * i : 64 * i + 64, cols].astype(F32)
                    swapped = jnp.where(low, pltpu.roll(a, PART - 32, 1), pltpu.roll(a, 32, 1))
                    turned = (a * cosine + swapped * sine).astype(BF16)
                    if g == 0:
                        qs[0, base : base + 64, cols] = turned
                    else:
                        kv[base : base + 64, cols] = turned
            kv[base : base + 64, HEAD : 2 * HEAD] = raw[2, 64 * i : 64 * i + 64, :]
        if p == 0:
            kv[LAT_KEYS : LAT_KEYS + CTX, 0:HEAD] = raw[1, 64 : 64 + CTX, :]
            kv[LAT_KEYS : LAT_KEYS + CTX, HEAD : 2 * HEAD] = raw[2, 64 : 64 + CTX, :]
        for d in (2, 1, 3):
            go(query_copy(p, d))
            go(key_copy(p, d))
            if p == 0:
                go(context_copy(d))

    def rows_of(p):
        return 64 * PASSES[p][0], 64 * len(PASSES[p])

    def query_copy(p, d):
        start, count = rows_of(p)
        return remote(
            qs.at[0, pl.ds(start, count)],
            qs.at[4 - d, pl.ds(start, count)],
            qsem_s.at[p, d],
            qsem_r.at[p, 4 - d],
            on_queries(d),
        )

    def key_copy(p, d):
        start, count = rows_of(p)
        return remote(
            kv.at[pl.ds(start, count)],
            kv.at[pl.ds((4 - d) * ROWS + start, count)],
            ksem_s.at[p, d],
            ksem_r.at[p, 4 - d],
            on_keys(d),
        )

    def context_copy(d):
        return remote(
            kv.at[pl.ds(LAT_KEYS, CTX)],
            kv.at[pl.ds(LAT_KEYS + (4 - d) * CTX, CTX)],
            csem_s.at[d],
            csem_r.at[4 - d],
            on_keys(d),
        )

    def slots_in(slots, halves=(0, 1)):
        for slot in slots:
            for h in halves:
                across(slot, h).wait_recv()

    slots_in(PASSES[0])
    step(0)
    relay(2, 1)
    slots_in(PASSES[1])
    step(1)
    relay(3, 0)
    relay(3, 1)
    slots_in(PASSES[2])
    step(2)
    relay(4, 0)
    slots_in(PASSES[3])
    step(3)
    slots_in(PASSES[4])
    step(4)
    loads[6].wait()
    go(remote(wout.at[0], wout.at[1], wsem.at[0], wsem.at[1], partner))

    for p in range(5):
        for d in (1, 2, 3):
            query_copy(p, d).wait_recv()
            key_copy(p, d).wait_recv()
    for d in (1, 2, 3):
        context_copy(d).wait_recv()

    lift = context_lift[0] * LOG2E
    column = lax.broadcasted_iota(jnp.int32, (TILE, PART), 1)

    def out_copies(j, half):
        rows = pl.ds(pl.multiple_of(half * TILE, TILE), TILE)
        to = on_queries(j)
        return (
            remote(
                outs.at[j, rows],
                outs_in.at[lax.rem(4 - j, 4), rows],
                osem_s.at[j, half],
                osem_r.at[lax.rem(4 - j, 4), half],
                to,
            ),
            remote(
                stats.at[j, half],
                stats_in.at[lax.rem(4 - j, 4), half],
                tsem_s.at[j, half],
                tsem_r.at[lax.rem(4 - j, 4), half],
                to,
            ),
        )

    def attend(i, carry):
        j = 3 - lax.div(i, 2)
        half = lax.rem(i, 2)
        start = pl.multiple_of(half * TILE, TILE)
        found = []
        for m in (0, 1):
            cols = slice(m * PART, (m + 1) * PART)
            q = qs[j, pl.ds(start, TILE), cols]
            s = lax.dot_general(
                q, kv[:, cols], (((1,), (1,)), ((), ())), preferred_element_type=F32
            )
            near = s[:, :LAT_KEYS]
            far = s[:, LAT_KEYS:] * SCALE2 + lift
            peak = jnp.maximum(
                jnp.max(near, axis=1, keepdims=True) * SCALE2, jnp.max(far, axis=1, keepdims=True)
            )
            near = jnp.exp2(near * SCALE2 - peak)
            far = jnp.exp2(far - peak)
            total = jnp.sum(near, axis=1, keepdims=True) + jnp.sum(far, axis=1, keepdims=True)
            o = jnp.dot(
                near.astype(BF16), kv[:LAT_KEYS, HEAD : 2 * HEAD], preferred_element_type=F32
            ) + jnp.dot(
                far.astype(BF16), kv[LAT_KEYS:, HEAD : 2 * HEAD], preferred_element_type=F32
            )
            outs[j, pl.ds(start, TILE), m * HEAD : (m + 1) * HEAD] = (o / total).astype(BF16)
            found += [peak, total]
        table = jnp.where(
            column == 0,
            found[0],
            jnp.where(column == 1, found[1], jnp.where(column == 2, found[2], found[3])),
        )
        stats[j, half] = table.T[:8, :]

        @pl.when(j > 0)
        def _():
            for copy in out_copies(j, half):
                copy.start()

        return carry

    lax.fori_loop(0, 8, attend, 0)

    for half in (0, 1):
        for j in (3, 2, 1):
            for copy in out_copies(j, half):
                copy.wait_recv()
        rows = pl.ds(half * TILE, TILE)
        tables = [stats[0, half]] + [stats_in[j, half] for j in (1, 2, 3)]
        turned = jnp.concatenate(tables + [jnp.zeros((96, TILE), F32)], axis=0).T
        means = []
        for m in (0, 1):
            peaks = [turned[:, 8 * j + 2 * m : 8 * j + 2 * m + 1] for j in range(4)]
            totals = [turned[:, 8 * j + 2 * m + 1 : 8 * j + 2 * m + 2] for j in range(4)]
            top = jnp.maximum(jnp.maximum(peaks[0], peaks[1]), jnp.maximum(peaks[2], peaks[3]))
            shares = [t * jnp.exp2(p - top) for p, t in zip(peaks, totals)]
            whole = (shares[0] + shares[1]) + (shares[2] + shares[3])
            cols = slice(m * HEAD, (m + 1) * HEAD)
            acc = outs[0, rows, cols].astype(F32) * (shares[0] / whole)
            for j in (1, 2, 3):
                acc += outs_in[j, rows, cols].astype(F32) * (shares[j] / whole)
            means.append(acc)
        difference = means[0] - lambdas[0] * means[1]
        spread = jnp.mean(jnp.square(difference), axis=1, keepdims=True)
        gain = jnp.concatenate([head_gain[0:1, :], head_gain[1:2, :]], axis=1)
        scaled = difference * lax.rsqrt(spread + EPSILON) * gain
        att[4 * half : 4 * half + 4] = scaled.astype(BF16).reshape(4, 2, OWN, HEAD)

    swap = remote(att.at[:, 1], att_in, asem.at[0], asem.at[1], partner)
    go(swap)
    swap.wait_recv()
    remote(wout.at[0], wout.at[1], wsem.at[0], wsem.at[1], partner).wait_recv()

    mine = att[:, 0].reshape(8 * OWN, HEAD)
    theirs = att_in[...].reshape(8 * OWN, HEAD)

    def multiply(n, carry):
        cols = pl.ds(pl.multiple_of(n * 512, 512), 512)
        got = jnp.dot(mine, wout[0, :, cols], preferred_element_type=F32)
        got += jnp.dot(theirs, wout[1, :, cols], preferred_element_type=F32)
        part[:, :, cols] = got.reshape(8, OWN, 512)
        return carry

    lax.fori_loop(0, 8, multiply, 0)

    def sum_slot(way, t):
        return 7 if t == 1 else 2 * (5 - t) if way == 0 else 2 * (5 - t) - 1

    def sum_copy(way, t, h):
        return remote(
            sum_out.at[way, t - 1, h],
            sum_in.at[way, t - 1, h],
            rs.at[way, t - 1, h],
            rr.at[way, t - 1, h],
            on_z(1 if way == 0 else -1),
        )

    def send_sum(way, t, h, add):
        slot = sum_slot(way, t)
        for n in range(4):
            cols = slice(n * 1024, (n + 1) * 1024)
            total = part[slot, 16 * h : 16 * h + 16, cols]
            if add:
                total = total + sum_in[way, t - 2, h, :, cols].astype(F32)
            sum_out[way, t - 1, h, :, cols] = total.astype(BF16)
        go(sum_copy(way, t, h))

    for way in (0, 1):
        send_sum(way, 1, way, False)
    for way in (0, 1):
        send_sum(way, 2, 1 - way, False)
    for t, turn in ((2, 0), (3, 1), (3, 0), (4, 1), (4, 0)):
        for way in (0, 1):
            h = turn if way == 0 else 1 - turn
            sum_copy(way, t - 1, h).wait_recv()
            send_sum(way, t, h, True)
    for turn in (1, 0):
        for way in (0, 1):
            sum_copy(way, 4, turn if way == 0 else 1 - turn).wait_recv()
    for h in (0, 1):
        rows = slice(16 * h, 16 * h + 16)
        for t in range(16):
            cols = slice(t * 256, (t + 1) * 256)
            mixture = part[0, rows, cols] + (
                sum_in[0, 3, h, :, cols].astype(F32) + sum_in[1, 3, h, :, cols].astype(F32)
            )
            gate = mod_all[t // 2, t % 2, 4:5, :]
            result[rows, cols] = (gx[0, rows, cols].astype(F32) + gate * mixture).astype(BF16)

    for copy in waits:
        copy.wait_send()
    for j in (1, 2, 3):
        for half in (0, 1):
            for copy in out_copies(j, half):
                copy.wait_send()


def shards(*args):
    (
        latent,
        context,
        condition,
        context_condition,
        modulation,
        query_weight,
        key_weight,
        value_weight,
        lambdas,
        context_lift,
        head_gain,
        output_weight,
    ) = args
    anywhere = pl.BlockSpec(memory_space=pl.ANY)
    inside = pl.BlockSpec(memory_space=pltpu.VMEM)
    scalar = pl.BlockSpec(memory_space=pltpu.SMEM)
    tables = rope_tables()
    dma = pltpu.SemaphoreType.DMA
    scratch = [
        pltpu.VMEM((8, 64, WIDTH), BF16),
        pltpu.VMEM((CTX, WIDTH), BF16),
        pltpu.VMEM((3, 256, 256), BF16),
        pltpu.VMEM((3, WIDTH, HEAD), BF16),
        pltpu.VMEM((128, WIDTH), BF16),
        pltpu.VMEM((4, 8, 256), F32),
        pltpu.VMEM((4, 8, 256), F32),
        pltpu.VMEM((8, 2, 8, 256), F32),
        pltpu.VMEM((3, 128, HEAD), BF16),
        pltpu.VMEM((4, ROWS, HEAD), BF16),
        pltpu.VMEM((KEYS, 2 * HEAD), BF16),
        pltpu.VMEM((4, ROWS, 2 * HEAD), BF16),
        pltpu.VMEM((4, ROWS, 2 * HEAD), BF16),
        pltpu.VMEM((4, 2, 8, TILE), F32),
        pltpu.VMEM((4, 2, 8, TILE), F32),
        pltpu.VMEM((8, 2, OWN, HEAD), BF16),
        pltpu.VMEM((8, OWN, HEAD), BF16),
        pltpu.VMEM((2, HEAD, WIDTH), BF16),
        pltpu.VMEM((8, OWN, WIDTH), F32),
        pltpu.VMEM((2, 4, 2, 16, WIDTH), BF16),
        pltpu.VMEM((2, 4, 2, 16, WIDTH), BF16),
        dma((7,)),
        dma((2, 4, 2)),
        dma((2, 4, 2)),
        dma((8, 2)),
        dma((8, 2)),
        dma((2, 4)),
        dma((2, 4)),
        dma((8,)),
        dma((8,)),
        dma((8,)),
        dma((8,)),
        dma((5, 4)),
        dma((5, 4)),
        dma((5, 4)),
        dma((5, 4)),
        dma((4,)),
        dma((4,)),
        dma((4, 2)),
        dma((4, 2)),
        dma((4, 2)),
        dma((4, 2)),
        dma((2,)),
        dma((2,)),
        dma((2, 4, 2)),
        dma((2, 4, 2)),
    ]
    return pl.pallas_call(
        body,
        out_shape=jax.ShapeDtypeStruct(latent.shape, BF16),
        in_specs=[
            anywhere,
            anywhere,
            inside,
            inside,
            anywhere,
            anywhere,
            anywhere,
            anywhere,
            scalar,
            scalar,
            inside,
            anywhere,
            inside,
            inside,
            inside,
            inside,
        ],
        out_specs=inside,
        scratch_shapes=scratch,
        compiler_params=pltpu.CompilerParams(
            collective_id=0, has_side_effects=True, vmem_limit_bytes=60 * 1024 * 1024
        ),
        name="layer",
    )(
        latent,
        context,
        condition.reshape(WIDTH // 128, 128),
        context_condition.reshape(WIDTH // 128, 128),
        modulation,
        query_weight,
        key_weight,
        value_weight,
        lambdas,
        context_lift,
        head_gain.reshape(2, 128),
        output_weight,
        *tables,
    )


def solution(mesh):
    split = Mesh(mesh.devices.reshape(4, 4, 8, 2), ("y", "x", "z", "c"))
    plane = ("y", "x")
    column = ("z", "c")
    every = ("y", "x", "z", "c")
    return jax.shard_map(
        shards,
        mesh=split,
        in_specs=(
            P(every, None),
            P(plane, None),
            P(),
            P(),
            P(None, plane, column),
            P(None, column),
            P(None, column),
            P(None, column),
            P(column),
            P(column),
            P(),
            P(column, None),
        ),
        out_specs=P(every, None),
        check_vma=False,
    )
```

```python
import functools
import math

import jax
import jax.numpy as jnp
import numpy as np
from jax import lax
from jax.experimental import pallas as pl
from jax.experimental.pallas import tpu as pltpu
from jax.sharding import Mesh
from jax.sharding import PartitionSpec as P

MESH = pl.DeviceIdType.MESH
F32 = jnp.float32
BF16 = jnp.bfloat16

WIDTH = 4096
GRID_W = 64
ROPE_BASE = 10000.0
EPSILON = 1e-05
HEAD = 256
PART = 128
LOG2E = math.log2(math.e)
SCALE2 = PART ** (-0.5) * LOG2E
ROWS = 512
OWN = 32
CTX = 32
MEMBERS = 4
LAT_KEYS = MEMBERS * ROWS
KEYS = LAT_KEYS + MEMBERS * CTX
TILE = 256
OFFSET = (0, -1, 1, -2, 2, -3, 3, 4)
PASSES = ((0,), (1, 2), (3, 4), (5, 6), (7,))


def rope_tables():
    quarter = PART // 2
    eighth = PART // 4
    inverse = np.float32(ROPE_BASE) ** (-np.arange(eighth, dtype=np.float32) / np.float32(eighth))
    inverse = inverse.astype(np.float32)
    sign = np.concatenate([-np.ones(eighth), np.ones(eighth)]).astype(np.float32)

    def pair(count):
        angles = np.arange(count, dtype=np.float32)[:, None] * np.concatenate([inverse, inverse])
        angles = angles.astype(np.float32).astype(np.float64)
        return np.cos(angles).astype(np.float32), (np.sin(angles) * sign).astype(np.float32)

    row_cos, row_sin = pair(8192 // GRID_W)
    col_cos, col_sin = pair(GRID_W)
    none = np.zeros_like(row_cos)
    row_cos, row_sin = (np.concatenate([t, none], axis=1) for t in (row_cos, row_sin))
    none = np.zeros_like(col_cos)
    col_cos, col_sin = (np.concatenate([none, t], axis=1) for t in (col_cos, col_sin))
    half = GRID_W // 2
    both = [np.stack([t, np.concatenate([t[half:], t[:half]])]) for t in (col_cos, col_sin)]
    return row_cos, row_sin, both[0], both[1]


def body(
    latent,
    context,
    condition,
    context_condition,
    modulation,
    query_weight,
    key_weight,
    value_weight,
    lambdas,
    context_lift,
    head_gain,
    output_weight,
    row_cos,
    row_sin,
    col_cos,
    col_sin,
    result,
    res,
    lat,
    cond,
    cond_ctx,
    rows_cos,
    rows_sin,
    cols_cos,
    cols_sin,
    gx,
    ctx,
    modw,
    weights,
    xn,
    mod_in,
    mod_all,
    raw,
    qs,
    kv,
    outs,
    outs_in,
    tab,
    stats,
    stats_in,
    att,
    att_in,
    wout,
    part,
    sum_out,
    sum_in,
    load_sem,
    xs,
    xr,
    ps,
    pr,
    ms,
    mr,
    zs,
    zr,
    qsem_s,
    qsem_r,
    ksem_s,
    ksem_r,
    csem_s,
    csem_r,
    osem_s,
    osem_r,
    tsem_s,
    tsem_r,
    asem,
    wsem,
    rs,
    rr,
):
    y, x, z, c = (lax.axis_index(a) for a in ("y", "x", "z", "c"))
    sp = y * 4 + x
    waits = []

    def remote(src, dst, send, recv, to):
        return pltpu.make_async_remote_copy(
            src_ref=src, dst_ref=dst, send_sem=send, recv_sem=recv, device_id=to, device_id_type=MESH
        )

    def go(copy):
        copy.start()
        waits.append(copy)

    partner = {"c": 1 - c}

    def on_plane(dy, dx):
        return {"y": lax.rem(y + dy, 4), "x": lax.rem(x + dx, 4)}

    def on_z(d):
        return {"z": lax.rem(z + d + 8, 8)}

    def on_queries(d):
        return {"y": lax.rem(y + d * c, 4), "x": lax.rem(x + d * (1 - c), 4)}

    def on_keys(d):
        return {"y": lax.rem(y + d * (1 - c), 4), "x": lax.rem(x + d * c, 4)}

    pairs = (
        (latent, lat),
        (condition, cond),
        (context_condition, cond_ctx),
        (modulation, modw),
        (context, ctx),
        (row_cos, rows_cos),
        (row_sin, rows_sin),
        (col_cos, cols_cos),
        (col_sin, cols_sin),
        (query_weight, weights.at[0]),
        (key_weight, weights.at[1]),
        (value_weight, weights.at[2]),
        (output_weight, wout.at[0]),
    )
    loads = [pltpu.make_async_copy(a, b, load_sem.at[i]) for i, (a, b) in enumerate(pairs)]
    for load in loads:
        load.start()

    barrier = pltpu.get_barrier_semaphore()
    plane = [(dy, dx) for dy in range(4) for dx in range(4) if dy or dx]
    plane.sort(key=lambda d: -(min(d[0], 4 - d[0]) + min(d[1], 4 - d[1])))
    column = [(dz, dc) for dz in (4, 3, 5, 2, 6, 1, 7, 0) for dc in (1, 0) if dz or dc]

    def on_column(dz, dc):
        return {"z": lax.rem(z + dz, 8), "c": 1 - c if dc else c}

    peers = [on_column(*d) for d in column] + [on_plane(*d) for d in plane]
    for peer in peers:
        pl.semaphore_signal(barrier, inc=1, device_id=peer, device_id_type=MESH)

    def centered(src, g):
        v = src[pl.ds(pl.multiple_of(g * 16, 16), 16), :].astype(F32)
        v = v - jnp.mean(v, axis=-1, keepdims=True)
        spread = jnp.mean(jnp.square(v), axis=-1, keepdims=True)
        return v * lax.rsqrt(spread + EPSILON)

    def own_group(g, carry):
        gx[0, pl.ds(pl.multiple_of(g * 16, 16), 16), :] = centered(lat, g).astype(BF16)
        return carry

    loads[0].wait()
    lax.fori_loop(0, OWN // 16, own_group, 0)
    pl.semaphore_wait(barrier, len(peers))

    def ring_slot(way, k):
        return 0 if k == 0 else 7 if k == 4 else 2 * k - 1 if way == 0 else 2 * k

    def ring_copy(way, k, h):
        rows = pl.ds(16 * h, 16)
        return remote(
            gx.at[ring_slot(way, k - 1), rows],
            gx.at[ring_slot(way, k), rows],
            xs.at[way, k - 1, h],
            xr.at[way, k - 1, h],
            on_z(1 if way == 0 else -1),
        )

    def across(slot, h):
        return remote(
            gx.at[slot, pl.ds(16 * h, 16)],
            gx.at[slot, pl.ds(OWN + 16 * h, 16)],
            ps.at[slot, h],
            pr.at[slot, h],
            partner,
        )

    def relay(k, turn):
        for way in (0, 1):
            h = turn if way == 0 else 1 - turn
            if k == 4 and turn == 1:
                continue
            ring_copy(way, k, h).wait_recv()
            if k < 3 or (k == 3 and turn == 0):
                go(ring_copy(way, k + 1, h))
            go(across(ring_slot(way, k), h))

    for turn in (0, 1):
        for way in (0, 1):
            go(ring_copy(way, 1, turn if way == 0 else 1 - turn))
    for h in (0, 1):
        go(across(0, h))

    def silu_rows(ref):
        halves = [ref[pl.ds(2 * sp + i, 1), :] for i in (0, 1)]
        v = jnp.concatenate(halves, axis=1)
        return (v / (1.0 + jnp.exp(-v))).astype(BF16).astype(F32)

    for load in loads[1:4]:
        load.wait()
    own = silu_rows(cond)
    other = silu_rows(cond_ctx)
    at_row = lax.broadcasted_iota(jnp.int32, (16, 256), 0)
    partial = jnp.zeros((16, 256), F32)
    for r in range(3):
        lhs = jnp.where(at_row == 2 * r, own, jnp.where(at_row == 2 * r + 1, other, 0.0))
        partial += jnp.dot(lhs.astype(BF16), modw[r], preferred_element_type=F32)
    def tile_of(first):
        rows = partial[first : first + 4]
        return jnp.concatenate([rows[:, :PART], rows[:, PART:]], axis=0)

    mod_in[0, 0] = tile_of(0)
    mod_in[0, 1] = tile_of(4)

    def mod_copy(dy, dx):
        there = ((4 - dy) % 4) * 4 + (4 - dx) % 4
        return remote(
            mod_in.at[0], mod_in.at[there], ms.at[dy * 4 + dx], mr.at[there], on_plane(dy, dx)
        )

    for d in plane:
        go(mod_copy(*d))
    for d in plane:
        mod_copy(*d).wait_recv()

    def total_of(which):
        lines = [
            (mod_in[4 * i, which] + mod_in[4 * i + 1, which])
            + (mod_in[4 * i + 2, which] + mod_in[4 * i + 3, which])
            for i in range(4)
        ]
        return (lines[0] + lines[1]) + (lines[2] + lines[3])

    def spread(which):
        mod_all[which, z, c] = total_of(which)
        slab = mod_all.at[which, z, c]
        for dz, dc in column:
            there = ((8 - dz) % 8) * 2 + dc
            at = dz * 2 + dc
            go(remote(slab, slab, zs.at[which, at], zr.at[which, there], on_column(dz, dc)))

    def gathered(which):
        for dz, dc in column:
            slab = mod_all.at[which, lax.rem(z + dz, 8), 1 - c if dc else c]
            at = dz * 2 + dc
            remote(slab, slab, zs.at[which, at], zr.at[which, at], on_column(dz, dc)).wait_recv()

    spread(0)
    relay(1, 0)
    relay(1, 1)
    relay(2, 0)
    gathered(0)

    def shift_scale(t, which):
        tile = mod_all.at[0, t // 4, (t // 2) % 2]
        row = 4 * (t % 2) + which
        return tile[row : row + 1, :], 1.0 + tile[row + 2 : row + 3, :], slice(t * PART, (t + 1) * PART)

    def context_group(g, carry):
        v = centered(ctx, g)
        for t in range(32):
            offset, scaling, cols = shift_scale(t, 1)
            done = v[:, cols] * scaling + offset
            xn[pl.ds(pl.multiple_of(64 + g * 16, 16), 16), cols] = done.astype(BF16)
        return carry

    def modulated(slots):
        for t in range(32):
            offset, scaling, cols = shift_scale(t, 0)
            for i, slot in enumerate(slots):
                done = gx[slot, :, cols].astype(F32) * scaling + offset
                xn[64 * i : 64 * i + 64, cols] = done.astype(BF16)

    lane = lax.broadcasted_iota(jnp.int32, (64, PART), 1)
    low = lax.rem(lane, 64) < 32

    def project(count):
        def one(g, carry):
            raw[g, pl.ds(0, count)] = jnp.dot(
                xn[pl.ds(0, count), :], weights[g], preferred_element_type=F32
            ).astype(BF16)
            return carry

        lax.fori_loop(0, 3, one, 0)

    def step(p):
        slots = PASSES[p]
        modulated(slots)
        count = 64 * len(slots)
        if p == 0:
            loads[4].wait()
            lax.fori_loop(0, CTX // 16, context_group, 0)
            count += CTX
            for load in loads[5:12]:
                load.wait()
        project(count)
        for i, slot in enumerate(slots):
            line = sp * 8 + lax.rem(z + OFFSET[slot] + 8, 8)
            cosine = cols_cos[c] + rows_cos[pl.ds(line, 1), :]
            sine = cols_sin[c] + rows_sin[pl.ds(line, 1), :]
            base = 64 * slot
            for g in (0, 1):
                for m in (0, 1):
                    cols = slice(m * PART, (m + 1) * PART)
                    a = raw[g, 64 * i : 64 * i + 64, cols].astype(F32)
                    swapped = jnp.where(low, pltpu.roll(a, PART - 32, 1), pltpu.roll(a, 32, 1))
                    turned = (a * cosine + swapped * sine).astype(BF16)
                    if g == 0:
                        qs[0, base : base + 64, cols] = turned
                    else:
                        kv[base : base + 64, cols] = turned
            kv[base : base + 64, HEAD : 2 * HEAD] = raw[2, 64 * i : 64 * i + 64, :]
        if p == 0:
            kv[LAT_KEYS : LAT_KEYS + CTX, 0:HEAD] = raw[1, 64 : 64 + CTX, :]
            kv[LAT_KEYS : LAT_KEYS + CTX, HEAD : 2 * HEAD] = raw[2, 64 : 64 + CTX, :]
        for d in near(p):
            if p == 0:
                go(context_copy(d))
            go(key_copy(p, d))
        for d in near(p):
            go(query_copy(p, d))

    def near(p):
        return (2, 1, 3) if p == 4 else (1, 3)

    def rows_of(p):
        return 64 * PASSES[p][0], 64 * len(PASSES[p])

    def query_copy(p, d):
        start, count = rows_of(p)
        return remote(
            qs.at[0, pl.ds(start, count)],
            qs.at[4 - d, pl.ds(start, count)],
            qsem_s.at[p, d],
            qsem_r.at[p, 4 - d],
            on_queries(d),
        )

    def query_relay(p, d):
        start, count = rows_of(p)
        rows = pl.ds(start + (0 if d == 1 else count // 2), count // 2)
        at = 0 if d == 1 else 2
        return remote(
            qs.at[4 - d, rows], qs.at[2, rows], qsem_s.at[5 + p, at], qsem_r.at[5 + p, at], on_queries(d)
        )

    def key_copy(p, d):
        start, count = rows_of(p)
        return remote(
            kv.at[pl.ds(start, count)],
            kv.at[pl.ds((4 - d) * ROWS + start, count)],
            ksem_s.at[p, d],
            ksem_r.at[p, 4 - d],
            on_keys(d),
        )

    def key_relay(p, d):
        start, count = rows_of(p)
        start, count = start + (0 if d == 1 else count // 2), count // 2
        at = 0 if d == 1 else 2
        return remote(
            kv.at[pl.ds((4 - d) * ROWS + start, count)],
            kv.at[pl.ds(2 * ROWS + start, count)],
            ksem_s.at[5 + p, at],
            ksem_r.at[5 + p, at],
            on_keys(d),
        )

    def context_copy(d):
        return remote(
            kv.at[pl.ds(LAT_KEYS, CTX)],
            kv.at[pl.ds(LAT_KEYS + (4 - d) * CTX, CTX)],
            csem_s.at[d],
            csem_r.at[4 - d],
            on_keys(d),
        )

    def context_relay(d):
        at = 0 if d == 1 else 2
        skip = 0 if d == 1 else CTX // 2
        return remote(
            kv.at[pl.ds(LAT_KEYS + (4 - d) * CTX + skip, CTX // 2)],
            kv.at[pl.ds(LAT_KEYS + 2 * CTX + skip, CTX // 2)],
            csem_s.at[4 + at],
            csem_r.at[4 + at],
            on_keys(d),
        )

    def hand_on(p):
        for d in (1, 3):
            if p == 0:
                context_copy(d).wait_recv()
                go(context_relay(d))
            key_copy(p, d).wait_recv()
            go(key_relay(p, d))
        for d in (1, 3):
            query_copy(p, d).wait_recv()
            go(query_relay(p, d))

    def slots_in(slots, halves=(0, 1)):
        for slot in slots:
            for h in halves:
                across(slot, h).wait_recv()

    slots_in(PASSES[0])
    step(0)
    relay(2, 1)
    slots_in(PASSES[1])
    step(1)
    relay(3, 0)
    hand_on(0)
    slots_in(PASSES[2])
    step(2)
    relay(3, 1)
    hand_on(1)
    relay(4, 0)
    spread(1)
    slots_in(PASSES[3])
    step(3)
    hand_on(2)
    slots_in(PASSES[4])
    step(4)
    loads[12].wait()
    go(remote(wout.at[0], wout.at[1], wsem.at[0], wsem.at[1], partner))
    hand_on(3)

    for p in range(5):
        for copy in (query_copy, key_copy):
            if p == 4:
                for d in (1, 2, 3):
                    copy(p, d).wait_recv()
        for relayed in (query_relay, key_relay):
            if p < 4:
                for d in (1, 3):
                    relayed(p, d).wait_recv()
    for d in (1, 3):
        context_relay(d).wait_recv()

    lift = context_lift[0] * LOG2E
    column_of = lax.broadcasted_iota(jnp.int32, (TILE, PART), 1)

    def attend(p, parts=(0, 1)):
        first, count = rows_of(p)
        parts = [i for i in parts if i < count // 64]

        for i in parts:
            rows = pl.ds(first + 64 * i, 64)
            found = []
            for m in (0, 1):
                cols = slice(m * PART, (m + 1) * PART)
                q = qs[:, rows, cols].reshape(TILE, PART)
                s = lax.dot_general(
                    q, kv[:, cols], (((1,), (1,)), ((), ())), preferred_element_type=F32
                )
                near_s = s[:, :LAT_KEYS]
                far = s[:, LAT_KEYS:] * SCALE2 + lift
                peak = jnp.maximum(
                    jnp.max(near_s, axis=1, keepdims=True) * SCALE2,
                    jnp.max(far, axis=1, keepdims=True),
                )
                near_s = jnp.exp2(near_s * SCALE2 - peak)
                far = jnp.exp2(far - peak)
                total = jnp.sum(near_s, axis=1, keepdims=True) + jnp.sum(far, axis=1, keepdims=True)
                o = jnp.dot(
                    near_s.astype(BF16), kv[:LAT_KEYS, HEAD : 2 * HEAD], preferred_element_type=F32
                ) + jnp.dot(
                    far.astype(BF16), kv[LAT_KEYS:, HEAD : 2 * HEAD], preferred_element_type=F32
                )
                o = (o / total).astype(BF16).reshape(MEMBERS, 64, HEAD)
                outs[:, rows, m * HEAD : (m + 1) * HEAD] = o
                found += [peak, total]
            table = jnp.where(
                column_of == 0,
                found[0],
                jnp.where(column_of == 1, found[1], jnp.where(column_of == 2, found[2], found[3])),
            )
            tab[i] = table.reshape(MEMBERS, 64, PART)
        if parts[-1] < count // 64 - 1:
            return
        for j in range(MEMBERS):
            second = tab[1, j] if count > 64 else jnp.zeros((64, PART), F32)
            stats[p, j] = jnp.concatenate([tab[0, j], second], axis=0).T[:8, :]
        for j in (2, 1, 3):
            for copy in out_copies(p, j):
                go(copy)

    def out_copies(p, j):
        start, count = rows_of(p)
        rows = pl.ds(start, count)
        to = on_queries(j)
        return (
            remote(
                outs.at[j, rows],
                outs_in.at[4 - j, rows],
                osem_s.at[p, j],
                osem_r.at[p, 4 - j],
                to,
            ),
            remote(
                stats.at[p, j],
                stats_in.at[p, 4 - j],
                tsem_s.at[p, j],
                tsem_r.at[p, 4 - j],
                to,
            ),
        )

    def swap(p):
        slots = pl.ds(PASSES[p][0], len(PASSES[p]))
        return remote(
            att.at[slots, 1], att_in.at[slots], asem.at[0, p], asem.at[1, p], partner
        )

    def combine(p):
        for j in (3, 1, 2):
            for copy in out_copies(p, j):
                copy.wait_recv()
        start, count = rows_of(p)
        rows = slice(start, start + count)
        tables = [stats[p, 0]] + [stats_in[p, j] for j in (1, 2, 3)]
        turned = jnp.concatenate(tables + [jnp.zeros((96, PART), F32)], axis=0).T[:count]
        means = []
        for m in (0, 1):
            peaks = [turned[:, 8 * j + 2 * m : 8 * j + 2 * m + 1] for j in range(4)]
            totals = [turned[:, 8 * j + 2 * m + 1 : 8 * j + 2 * m + 2] for j in range(4)]
            top = jnp.maximum(jnp.maximum(peaks[0], peaks[1]), jnp.maximum(peaks[2], peaks[3]))
            shares = [t * jnp.exp2(k - top) for k, t in zip(peaks, totals)]
            whole = (shares[0] + shares[1]) + (shares[2] + shares[3])
            cols = slice(m * HEAD, (m + 1) * HEAD)
            acc = outs[0, rows, cols].astype(F32) * (shares[0] / whole)
            for j in (1, 2, 3):
                acc += outs_in[j, rows, cols].astype(F32) * (shares[j] / whole)
            means.append(acc)
        difference = means[0] - lambdas[0] * means[1]
        spread = jnp.mean(jnp.square(difference), axis=1, keepdims=True)
        gain = jnp.concatenate([head_gain[0:1, :], head_gain[1:2, :]], axis=1)
        scaled = difference * lax.rsqrt(spread + EPSILON) * gain
        slot, many = PASSES[p][0], len(PASSES[p])
        att[slot : slot + many] = scaled.astype(BF16).reshape(many, 2, OWN, HEAD)
        go(swap(p))

    def multiply(p):
        swap(p).wait_recv()
        slot, many = PASSES[p][0], len(PASSES[p])
        mine = att[slot : slot + many, 0].reshape(many * OWN, HEAD)
        theirs = att_in[slot : slot + many].reshape(many * OWN, HEAD)
        for n in range(2):
            cols = slice(n * 2048, (n + 1) * 2048)
            got = jnp.dot(mine, wout[0, :, cols], preferred_element_type=F32)
            got += jnp.dot(theirs, wout[1, :, cols], preferred_element_type=F32)
            part[slot : slot + many, :, cols] = got.reshape(many, OWN, 2048)

    def sum_slot(way, t):
        return 7 if t == 1 else 2 * (5 - t) if way == 0 else 2 * (5 - t) - 1

    def sum_copy(way, t, h):
        return remote(
            sum_out.at[way, t - 1, h],
            sum_in.at[way, t - 1, h],
            rs.at[way, t - 1, h],
            rr.at[way, t - 1, h],
            on_z(1 if way == 0 else -1),
        )

    def send_sum(way, t, h, add):
        slot = sum_slot(way, t)
        for n in range(4):
            cols = slice(n * 1024, (n + 1) * 1024)
            total = part[slot, 16 * h : 16 * h + 16, cols]
            if add:
                total = total + sum_in[way, t - 2, h, :, cols].astype(F32)
            sum_out[way, t - 1, h, :, cols] = total.astype(BF16)
        go(sum_copy(way, t, h))

    def add_on(t, turns):
        for turn in turns:
            for way in (0, 1):
                h = turn if way == 0 else 1 - turn
                sum_copy(way, t - 1, h).wait_recv()
                send_sum(way, t, h, True)

    attend(4)
    attend(3)
    combine(4)
    attend(2, (0,))
    remote(wout.at[0], wout.at[1], wsem.at[0], wsem.at[1], partner).wait_recv()
    multiply(4)
    for way in (0, 1):
        send_sum(way, 1, way, False)
    attend(2, (1,))
    combine(3)
    attend(1, (0,))
    multiply(3)
    for way in (0, 1):
        send_sum(way, 2, 1 - way, False)
    add_on(2, (0,))
    attend(1, (1,))
    combine(2)
    attend(0)
    multiply(2)
    add_on(3, (1, 0))
    combine(1)
    combine(0)
    multiply(1)
    add_on(4, (1, 0))
    multiply(0)
    gathered(1)
    for turn in (1, 0):
        for way in (0, 1):
            sum_copy(way, 4, turn if way == 0 else 1 - turn).wait_recv()
    for h in (0, 1):
        rows = slice(16 * h, 16 * h + 16)
        for t in range(32):
            cols = slice(t * PART, (t + 1) * PART)
            mixture = part[0, rows, cols] + (
                sum_in[0, 3, h, :, cols].astype(F32) + sum_in[1, 3, h, :, cols].astype(F32)
            )
            row = 4 * (t % 2)
            gate = mod_all[1, t // 4, (t // 2) % 2, row : row + 1, :]
            res[rows, cols] = (lat[rows, cols].astype(F32) + gate * mixture).astype(BF16)

    store = pltpu.make_async_copy(res, result, load_sem.at[13])
    store.start()
    for copy in waits:
        copy.wait_send()
    store.wait()


def shards(*args):
    (
        latent,
        context,
        condition,
        context_condition,
        modulation,
        query_weight,
        key_weight,
        value_weight,
        lambdas,
        context_lift,
        head_gain,
        output_weight,
    ) = args
    anywhere = pl.BlockSpec(memory_space=pl.ANY)
    inside = pl.BlockSpec(memory_space=pltpu.VMEM)
    scalar = pl.BlockSpec(memory_space=pltpu.SMEM)
    tables = rope_tables()
    dma = pltpu.SemaphoreType.DMA
    scratch = [
        pltpu.VMEM((OWN, WIDTH), BF16),
        pltpu.VMEM((OWN, WIDTH), BF16),
        pltpu.VMEM((WIDTH // 128, 128), F32),
        pltpu.VMEM((WIDTH // 128, 128), F32),
        pltpu.VMEM((8192 // GRID_W, PART), F32),
        pltpu.VMEM((8192 // GRID_W, PART), F32),
        pltpu.VMEM((2, GRID_W, PART), F32),
        pltpu.VMEM((2, GRID_W, PART), F32),
        pltpu.VMEM((8, 64, WIDTH), BF16),
        pltpu.VMEM((CTX, WIDTH), BF16),
        pltpu.VMEM((3, 256, 256), BF16),
        pltpu.VMEM((3, WIDTH, HEAD), BF16),
        pltpu.VMEM((128, WIDTH), BF16),
        pltpu.VMEM((16, 2, 8, PART), F32),
        pltpu.VMEM((2, 8, 2, 8, PART), F32),
        pltpu.VMEM((3, 128, HEAD), BF16),
        pltpu.VMEM((4, ROWS, HEAD), BF16),
        pltpu.VMEM((KEYS, 2 * HEAD), BF16),
        pltpu.VMEM((4, ROWS, 2 * HEAD), BF16),
        pltpu.VMEM((4, ROWS, 2 * HEAD), BF16),
        pltpu.VMEM((2, MEMBERS, 64, PART), F32),
        pltpu.VMEM((5, MEMBERS, 8, PART), F32),
        pltpu.VMEM((5, MEMBERS, 8, PART), F32),
        pltpu.VMEM((8, 2, OWN, HEAD), BF16),
        pltpu.VMEM((8, OWN, HEAD), BF16),
        pltpu.VMEM((2, HEAD, WIDTH), BF16),
        pltpu.VMEM((8, OWN, WIDTH), F32),
        pltpu.VMEM((2, 4, 2, 16, WIDTH), BF16),
        pltpu.VMEM((2, 4, 2, 16, WIDTH), BF16),
        dma((14,)),
        dma((2, 4, 2)),
        dma((2, 4, 2)),
        dma((8, 2)),
        dma((8, 2)),
        dma((16,)),
        dma((16,)),
        dma((2, 16)),
        dma((2, 16)),
        dma((10, 4)),
        dma((10, 4)),
        dma((10, 4)),
        dma((10, 4)),
        dma((8,)),
        dma((8,)),
        dma((5, 4)),
        dma((5, 4)),
        dma((5, 4)),
        dma((5, 4)),
        dma((2, 5)),
        dma((2,)),
        dma((2, 4, 2)),
        dma((2, 4, 2)),
    ]
    return pl.pallas_call(
        body,
        out_shape=jax.ShapeDtypeStruct(latent.shape, BF16),
        in_specs=[anywhere] * 8 + [scalar, scalar, inside] + [anywhere] * 5,
        out_specs=anywhere,
        scratch_shapes=scratch,
        compiler_params=pltpu.CompilerParams(
            collective_id=0, has_side_effects=True, vmem_limit_bytes=60 * 1024 * 1024
        ),
        name="layer",
    )(
        latent,
        context,
        condition.reshape(WIDTH // 128, 128),
        context_condition.reshape(WIDTH // 128, 128),
        modulation,
        query_weight,
        key_weight,
        value_weight,
        lambdas,
        context_lift,
        head_gain.reshape(2, 128),
        output_weight,
        *tables,
    )


def solution(mesh):
    split = Mesh(mesh.devices.reshape(4, 4, 8, 2), ("y", "x", "z", "c"))
    plane = ("y", "x")
    column = ("z", "c")
    every = ("y", "x", "z", "c")
    return jax.shard_map(
        shards,
        mesh=split,
        in_specs=(
            P(every, None),
            P(plane, None),
            P(),
            P(),
            P(None, plane, column),
            P(None, column),
            P(None, column),
            P(None, column),
            P(column),
            P(column),
            P(),
            P(column, None),
        ),
        out_specs=P(every, None),
        check_vma=False,
    )
```

```python
import functools
import math

import jax
import jax.numpy as jnp
import numpy as np
from jax import lax
from jax.experimental import pallas as pl
from jax.experimental.pallas import tpu as pltpu
from jax.sharding import Mesh
from jax.sharding import PartitionSpec as P

MESH = pl.DeviceIdType.MESH
F32 = jnp.float32
BF16 = jnp.bfloat16

WIDTH = 4096
GRID_W = 64
ROPE_BASE = 10000.0
EPSILON = 1e-05
HEAD = 256
PART = 128
LOG2E = math.log2(math.e)
SCALE2 = PART ** (-0.5) * LOG2E
ROWS = 512
OWN = 32
CTX = 32
MEMBERS = 4
LAT_KEYS = MEMBERS * ROWS
KEYS = LAT_KEYS + MEMBERS * CTX
TILE = 256
OFFSET = (0, -1, 1, -2, 2, -3, 3, 4)
PASSES = ((0,), (1, 2), (3, 4), (5, 6), (7,))


def rope_tables():
    quarter = PART // 2
    eighth = PART // 4
    inverse = np.float32(ROPE_BASE) ** (-np.arange(eighth, dtype=np.float32) / np.float32(eighth))
    inverse = inverse.astype(np.float32)
    sign = np.concatenate([-np.ones(eighth), np.ones(eighth)]).astype(np.float32)

    def pair(count):
        angles = np.arange(count, dtype=np.float32)[:, None] * np.concatenate([inverse, inverse])
        angles = angles.astype(np.float32).astype(np.float64)
        return np.cos(angles).astype(np.float32), (np.sin(angles) * sign).astype(np.float32)

    row_cos, row_sin = pair(8192 // GRID_W)
    col_cos, col_sin = pair(GRID_W)
    none = np.zeros_like(row_cos)
    row_cos, row_sin = (np.concatenate([t, none], axis=1) for t in (row_cos, row_sin))
    none = np.zeros_like(col_cos)
    col_cos, col_sin = (np.concatenate([none, t], axis=1) for t in (col_cos, col_sin))
    half = GRID_W // 2
    both = [np.stack([t, np.concatenate([t[half:], t[:half]])]) for t in (col_cos, col_sin)]
    return row_cos, row_sin, both[0], both[1]


def body(
    latent,
    context,
    condition,
    context_condition,
    modulation,
    query_weight,
    key_weight,
    value_weight,
    lambdas,
    context_lift,
    head_gain,
    output_weight,
    row_cos,
    row_sin,
    col_cos,
    col_sin,
    result,
    res,
    lat,
    cond,
    cond_ctx,
    rows_cos,
    rows_sin,
    cols_cos,
    cols_sin,
    gx,
    ctx,
    modw,
    weights,
    xn,
    mod_in,
    mod_all,
    raw,
    qs,
    kv,
    outs,
    outs_in,
    tab,
    stats,
    stats_in,
    att,
    att_in,
    wout,
    part,
    sum_out,
    sum_in,
    load_sem,
    sent,
    xr,
    pr,
    mr,
    qr,
    kr,
    outs_r,
    stats_r,
    att_r,
    wout_r,
    rr,
):
    y, x, z, c = (lax.axis_index(a) for a in ("y", "x", "z", "c"))
    sp = y * 4 + x
    def remote(src, dst, send, recv, to):
        return pltpu.make_async_remote_copy(
            src_ref=src, dst_ref=dst, send_sem=send, recv_sem=recv, device_id=to, device_id_type=MESH
        )

    def go(copy):
        copy.start()

    def arrived(ref, semaphore):
        pltpu.make_async_copy(ref, ref, semaphore).wait()

    partner = {"c": 1 - c}

    def on_plane(dy, dx):
        return {"y": lax.rem(y + dy, 4), "x": lax.rem(x + dx, 4)}

    def on_z(d):
        return {"z": lax.rem(z + d + 8, 8)}

    def on_queries(d):
        return {"y": lax.rem(y + d * c, 4), "x": lax.rem(x + d * (1 - c), 4)}

    def on_keys(d):
        return {"y": lax.rem(y + d * (1 - c), 4), "x": lax.rem(x + d * c, 4)}

    pairs = (
        (latent, lat),
        (condition, cond),
        (context_condition, cond_ctx),
        (modulation, modw),
        (context, ctx),
        (row_cos, rows_cos),
        (row_sin, rows_sin),
        (col_cos, cols_cos),
        (col_sin, cols_sin),
        (query_weight, weights.at[0]),
        (key_weight, weights.at[1]),
        (value_weight, weights.at[2]),
        (output_weight, wout.at[0]),
    )
    loads = [pltpu.make_async_copy(a, b, load_sem.at[i]) for i, (a, b) in enumerate(pairs)]
    for load in loads:
        load.start()

    barrier = pltpu.get_barrier_semaphore()
    plane = [(dy, dx) for dy in range(4) for dx in range(4) if dy or dx]
    plane.sort(key=lambda d: -(min(d[0], 4 - d[0]) + min(d[1], 4 - d[1])))
    column = [(dz, dc) for dz in (4, 3, 5, 2, 6, 1, 7, 0) for dc in (1, 0) if dz or dc]

    def on_column(dz, dc):
        return {"z": lax.rem(z + dz, 8), "c": 1 - c if dc else c}

    peers = [on_column(*d) for d in column] + [on_plane(*d) for d in plane]
    for peer in peers:
        pl.semaphore_signal(barrier, inc=1, device_id=peer, device_id_type=MESH)

    def centered(src, g):
        v = src[pl.ds(pl.multiple_of(g * 16, 16), 16), :].astype(F32)
        v = v - jnp.mean(v, axis=-1, keepdims=True)
        spread = jnp.mean(jnp.square(v), axis=-1, keepdims=True)
        return v * lax.rsqrt(spread + EPSILON)

    def own_group(g, carry):
        gx[0, pl.ds(pl.multiple_of(g * 16, 16), 16), :] = centered(lat, g).astype(BF16)
        return carry

    loads[0].wait()
    lax.fori_loop(0, OWN // 16, own_group, 0)
    pl.semaphore_wait(barrier, len(peers))

    def ring_slot(way, k):
        return 0 if k == 0 else 7 if k == 4 else 2 * k - 1 if way == 0 else 2 * k

    def ring_copy(way, k, h):
        rows = pl.ds(16 * h, 16)
        return remote(
            gx.at[ring_slot(way, k - 1), rows],
            gx.at[ring_slot(way, k), rows],
            sent.at[0],
            xr.at[way, 2 * (k - 1) + (h if k < 4 else 0)],
            on_z(1 if way == 0 else -1),
        )

    def across(slot, h):
        return remote(
            gx.at[slot, pl.ds(16 * h, 16)],
            gx.at[slot, pl.ds(OWN + 16 * h, 16)],
            sent.at[1],
            pr.at[slot],
            partner,
        )

    def relay(k, turn):
        for way in (0, 1):
            h = turn if way == 0 else 1 - turn
            if k == 4 and turn == 1:
                continue
            ring_copy(way, k, h).wait_recv()
            if k < 3 or (k == 3 and turn == 0):
                go(ring_copy(way, k + 1, h))
            go(across(ring_slot(way, k), h))

    for turn in (0, 1):
        for way in (0, 1):
            go(ring_copy(way, 1, turn if way == 0 else 1 - turn))
    for h in (0, 1):
        go(across(0, h))

    def silu_rows(ref):
        halves = [ref[pl.ds(2 * sp + i, 1), :] for i in (0, 1)]
        v = jnp.concatenate(halves, axis=1)
        return (v / (1.0 + jnp.exp(-v))).astype(BF16).astype(F32)

    for load in loads[1:4]:
        load.wait()
    own = silu_rows(cond)
    other = silu_rows(cond_ctx)
    at_row = lax.broadcasted_iota(jnp.int32, (16, 256), 0)
    partial = jnp.zeros((16, 256), F32)
    for r in range(3):
        lhs = jnp.where(at_row == 2 * r, own, jnp.where(at_row == 2 * r + 1, other, 0.0))
        partial += jnp.dot(lhs.astype(BF16), modw[r], preferred_element_type=F32)
    def tile_of(first):
        rows = partial[first : first + 4]
        return jnp.concatenate([rows[:, :PART], rows[:, PART:]], axis=0)

    mod_in[0, 0] = tile_of(0)
    mod_in[0, 1] = tile_of(4)

    def mod_copy(dy, dx):
        there = ((4 - dy) % 4) * 4 + (4 - dx) % 4
        return remote(
            mod_in.at[0], mod_in.at[there], sent.at[2], mr.at[0], on_plane(dy, dx)
        )

    for d in plane:
        go(mod_copy(*d))
    arrived(mod_in.at[pl.ds(1, 15)], mr.at[0])

    def total_of(which):
        lines = [
            (mod_in[4 * i, which] + mod_in[4 * i + 1, which])
            + (mod_in[4 * i + 2, which] + mod_in[4 * i + 3, which])
            for i in range(4)
        ]
        return (lines[0] + lines[1]) + (lines[2] + lines[3])

    def spread(which):
        mod_all[which, 2 * z + c] = total_of(which)
        slab = mod_all.at[which, 2 * z + c]
        for d in column:
            go(remote(slab, slab, sent.at[3 + which], mr.at[1 + which], on_column(*d)))

    def gathered(which):
        arrived(mod_all.at[which, pl.ds(0, 15)], mr.at[1 + which])

    spread(0)
    relay(1, 0)
    relay(1, 1)
    relay(2, 0)
    gathered(0)

    def shift_scale(t, which):
        tile = mod_all.at[0, t // 2]
        row = 4 * (t % 2) + which
        return tile[row : row + 1, :], 1.0 + tile[row + 2 : row + 3, :], slice(t * PART, (t + 1) * PART)

    def context_group(g, carry):
        v = centered(ctx, g)
        for t in range(32):
            offset, scaling, cols = shift_scale(t, 1)
            done = v[:, cols] * scaling + offset
            xn[pl.ds(pl.multiple_of(64 + g * 16, 16), 16), cols] = done.astype(BF16)
        return carry

    def modulated(slots):
        for t in range(32):
            offset, scaling, cols = shift_scale(t, 0)
            for i, slot in enumerate(slots):
                done = gx[slot, :, cols].astype(F32) * scaling + offset
                xn[64 * i : 64 * i + 64, cols] = done.astype(BF16)

    lane = lax.broadcasted_iota(jnp.int32, (64, PART), 1)
    low = lax.rem(lane, 64) < 32

    def project(count, first, last):
        def one(g, carry):
            raw[g, pl.ds(0, count)] = jnp.dot(
                xn[pl.ds(0, count), :], weights[g], preferred_element_type=F32
            ).astype(BF16)
            return carry

        lax.fori_loop(first, last, one, 0)

    def step(p):
        slots = PASSES[p]
        modulated(slots)
        count = 64 * len(slots)
        latent_count = count
        if p == 0:
            loads[4].wait()
            lax.fori_loop(0, CTX // 16, context_group, 0)
            count += CTX
            for load in loads[5:12]:
                load.wait()

        def turn(g):
            for i, slot in enumerate(slots):
                line = sp * 8 + lax.rem(z + OFFSET[slot] + 8, 8)
                cosine = cols_cos[c] + rows_cos[pl.ds(line, 1), :]
                sine = cols_sin[c] + rows_sin[pl.ds(line, 1), :]
                base = 64 * slot
                for m in (0, 1):
                    cols = slice(m * PART, (m + 1) * PART)
                    a = raw[g, 64 * i : 64 * i + 64, cols].astype(F32)
                    swapped = jnp.where(low, pltpu.roll(a, PART - 32, 1), pltpu.roll(a, 32, 1))
                    turned = (a * cosine + swapped * sine).astype(BF16)
                    if g == 0:
                        qs[0, base : base + 64, cols] = turned
                    else:
                        kv[base : base + 64, cols] = turned

        project(count, 1, 3)
        turn(1)
        base = 64 * slots[0]
        kv[base : base + latent_count, HEAD : 2 * HEAD] = raw[2, :latent_count, :]
        if p == 0:
            kv[LAT_KEYS : LAT_KEYS + CTX, 0:HEAD] = raw[1, 64 : 64 + CTX, :]
            kv[LAT_KEYS : LAT_KEYS + CTX, HEAD : 2 * HEAD] = raw[2, 64 : 64 + CTX, :]
        for d in near(p):
            if p == 0:
                go(context_copy(d))
            go(key_copy(p, d))
        project(latent_count, 0, 1)
        turn(0)
        for d in near(p):
            go(query_copy(p, d))

    def near(p):
        return (2, 1, 3) if p == 4 else (1, 3)

    def rows_of(p):
        return 64 * PASSES[p][0], 64 * len(PASSES[p])

    def query_copy(p, d):
        start, count = rows_of(p)
        return remote(
            qs.at[0, pl.ds(start, count)],
            qs.at[4 - d, pl.ds(start, count)],
            sent.at[5],
            qr.at[p],
            on_queries(d),
        )

    def query_relay(p, d):
        start, count = rows_of(p)
        rows = pl.ds(start + (0 if d == 1 else count // 2), count // 2)
        return remote(
            qs.at[4 - d, rows], qs.at[2, rows], sent.at[5], qr.at[5 + p], on_queries(d)
        )

    def key_copy(p, d):
        start, count = rows_of(p)
        return remote(
            kv.at[pl.ds(start, count)],
            kv.at[pl.ds((4 - d) * ROWS + start, count)],
            sent.at[6],
            kr.at[p],
            on_keys(d),
        )

    def key_relay(p, d):
        start, count = rows_of(p)
        start, count = start + (0 if d == 1 else count // 2), count // 2
        return remote(
            kv.at[pl.ds((4 - d) * ROWS + start, count)],
            kv.at[pl.ds(2 * ROWS + start, count)],
            sent.at[6],
            kr.at[5 + p],
            on_keys(d),
        )

    def context_copy(d):
        return remote(
            kv.at[pl.ds(LAT_KEYS, CTX)],
            kv.at[pl.ds(LAT_KEYS + (4 - d) * CTX, CTX)],
            sent.at[6],
            kr.at[0],
            on_keys(d),
        )

    def context_relay(d):
        skip = 0 if d == 1 else CTX // 2
        return remote(
            kv.at[pl.ds(LAT_KEYS + (4 - d) * CTX + skip, CTX // 2)],
            kv.at[pl.ds(LAT_KEYS + 2 * CTX + skip, CTX // 2)],
            sent.at[6],
            kr.at[5],
            on_keys(d),
        )

    def rows_in(p, share):
        return rows_of(p)[1] * share + (CTX * share if p == 0 else 0)

    def hand_on(p):
        arrived(kv.at[pl.ds(0, rows_in(p, 2))], kr.at[p])
        for d in (1, 3):
            if p == 0:
                go(context_relay(d))
            go(key_relay(p, d))
        arrived(qs.at[pl.ds(0, 2), pl.ds(0, rows_of(p)[1])], qr.at[p])
        for d in (1, 3):
            go(query_relay(p, d))

    def slots_in(slots):
        for slot in slots:
            arrived(gx.at[slot, pl.ds(0, OWN)], pr.at[slot])

    slots_in(PASSES[0])
    step(0)
    relay(2, 1)
    slots_in(PASSES[1])
    step(1)
    relay(3, 0)
    hand_on(0)
    slots_in(PASSES[2])
    step(2)
    relay(3, 1)
    hand_on(1)
    slots_in(PASSES[3])
    step(3)
    relay(4, 0)
    hand_on(2)
    slots_in(PASSES[4])
    step(4)
    spread(1)
    loads[12].wait()
    go(remote(wout.at[0], wout.at[1], sent.at[11], wout_r, partner))
    hand_on(3)

    for p in range(4):
        arrived(kv.at[pl.ds(0, rows_in(p, 1))], kr.at[5 + p])
        arrived(qs.at[0, pl.ds(0, rows_of(p)[1])], qr.at[5 + p])
    arrived(kv.at[pl.ds(0, rows_in(4, 3))], kr.at[4])
    arrived(qs.at[pl.ds(0, 3), pl.ds(0, rows_of(4)[1])], qr.at[4])

    lift = context_lift[0] * LOG2E
    column_of = lax.broadcasted_iota(jnp.int32, (TILE, PART), 1)

    def attend(p, parts=(0, 1)):
        first, count = rows_of(p)
        parts = [i for i in parts if i < count // 64]

        for i in parts:
            rows = pl.ds(first + 64 * i, 64)
            found = []
            for m in (0, 1):
                cols = slice(m * PART, (m + 1) * PART)
                q = qs[:, rows, cols].reshape(TILE, PART)
                s = lax.dot_general(
                    q, kv[:, cols], (((1,), (1,)), ((), ())), preferred_element_type=F32
                )
                near_s = s[:, :LAT_KEYS]
                far = s[:, LAT_KEYS:] * SCALE2 + lift
                peak = jnp.maximum(
                    jnp.max(near_s, axis=1, keepdims=True) * SCALE2,
                    jnp.max(far, axis=1, keepdims=True),
                )
                near_s = jnp.exp2(near_s * SCALE2 - peak)
                far = jnp.exp2(far - peak)
                total = jnp.sum(near_s, axis=1, keepdims=True) + jnp.sum(far, axis=1, keepdims=True)
                o = jnp.dot(
                    near_s.astype(BF16), kv[:LAT_KEYS, HEAD : 2 * HEAD], preferred_element_type=F32
                ) + jnp.dot(
                    far.astype(BF16), kv[LAT_KEYS:, HEAD : 2 * HEAD], preferred_element_type=F32
                )
                o = (o / total).astype(BF16).reshape(MEMBERS, 64, HEAD)
                outs[:, rows, m * HEAD : (m + 1) * HEAD] = o
                found += [peak, total]
            table = jnp.where(
                column_of == 0,
                found[0],
                jnp.where(column_of == 1, found[1], jnp.where(column_of == 2, found[2], found[3])),
            )
            tab[i] = table.reshape(MEMBERS, 64, PART)
        if parts[-1] < count // 64 - 1:
            return
        for j in range(MEMBERS):
            second = tab[1, j] if count > 64 else jnp.zeros((64, PART), F32)
            stats[p, j] = jnp.concatenate([tab[0, j], second], axis=0).T[:8, :]
        for j in (2, 1, 3):
            for copy in out_copies(p, j):
                go(copy)

    def out_copies(p, j):
        start, count = rows_of(p)
        rows = pl.ds(start, count)
        to = on_queries(j)
        return (
            remote(
                outs.at[j, rows],
                outs_in.at[4 - j, rows],
                sent.at[7],
                outs_r.at[p],
                to,
            ),
            remote(
                stats.at[p, j],
                stats_in.at[p, 4 - j],
                sent.at[8],
                stats_r.at[p],
                to,
            ),
        )

    def swap(p):
        slots = pl.ds(PASSES[p][0], len(PASSES[p]))
        return remote(
            att.at[slots, 1], att_in.at[slots], sent.at[9], att_r.at[p], partner
        )

    def combine(p):
        start, count = rows_of(p)
        arrived(outs_in.at[pl.ds(1, 3), pl.ds(start, count)], outs_r.at[p])
        arrived(stats_in.at[p, pl.ds(1, 3)], stats_r.at[p])
        rows = slice(start, start + count)
        tables = [stats[p, 0]] + [stats_in[p, j] for j in (1, 2, 3)]
        turned = jnp.concatenate(tables + [jnp.zeros((96, PART), F32)], axis=0).T[:count]
        means = []
        for m in (0, 1):
            peaks = [turned[:, 8 * j + 2 * m : 8 * j + 2 * m + 1] for j in range(4)]
            totals = [turned[:, 8 * j + 2 * m + 1 : 8 * j + 2 * m + 2] for j in range(4)]
            top = jnp.maximum(jnp.maximum(peaks[0], peaks[1]), jnp.maximum(peaks[2], peaks[3]))
            shares = [t * jnp.exp2(k - top) for k, t in zip(peaks, totals)]
            whole = (shares[0] + shares[1]) + (shares[2] + shares[3])
            cols = slice(m * HEAD, (m + 1) * HEAD)
            acc = outs[0, rows, cols].astype(F32) * (shares[0] / whole)
            for j in (1, 2, 3):
                acc += outs_in[j, rows, cols].astype(F32) * (shares[j] / whole)
            means.append(acc)
        difference = means[0] - lambdas[0] * means[1]
        spread = jnp.mean(jnp.square(difference), axis=1, keepdims=True)
        gain = jnp.concatenate([head_gain[0:1, :], head_gain[1:2, :]], axis=1)
        scaled = difference * lax.rsqrt(spread + EPSILON) * gain
        slot, many = PASSES[p][0], len(PASSES[p])
        att[slot : slot + many] = scaled.astype(BF16).reshape(many, 2, OWN, HEAD)
        go(swap(p))

    def multiply(p):
        swap(p).wait_recv()
        slot, many = PASSES[p][0], len(PASSES[p])
        mine = att[slot : slot + many, 0].reshape(many * OWN, HEAD)
        theirs = att_in[slot : slot + many].reshape(many * OWN, HEAD)
        for n in range(2):
            cols = slice(n * 2048, (n + 1) * 2048)
            got = jnp.dot(mine, wout[0, :, cols], preferred_element_type=F32)
            got += jnp.dot(theirs, wout[1, :, cols], preferred_element_type=F32)
            part[slot : slot + many, :, cols] = got.reshape(many, OWN, 2048)

    def sum_slot(way, t):
        return 7 if t == 1 else 2 * (5 - t) if way == 0 else 2 * (5 - t) - 1

    def sum_copy(way, t, h):
        return remote(
            sum_out.at[way, t - 1, h],
            sum_in.at[way, t - 1, h],
            sent.at[10],
            rr.at[way, 0 if t == 1 else 2 * t - 3 + h],
            on_z(1 if way == 0 else -1),
        )

    def send_sum(way, t, h, add):
        slot = sum_slot(way, t)
        for n in range(4):
            cols = slice(n * 1024, (n + 1) * 1024)
            total = part[slot, 16 * h : 16 * h + 16, cols]
            if add:
                total = total + sum_in[way, t - 2, h, :, cols].astype(F32)
            sum_out[way, t - 1, h, :, cols] = total.astype(BF16)
        go(sum_copy(way, t, h))

    def add_on(t, turns):
        for turn in turns:
            for way in (0, 1):
                h = turn if way == 0 else 1 - turn
                sum_copy(way, t - 1, h).wait_recv()
                send_sum(way, t, h, True)

    attend(4)
    attend(3)
    combine(4)
    attend(2, (0,))
    remote(wout.at[0], wout.at[1], sent.at[11], wout_r, partner).wait_recv()
    multiply(4)
    for way in (0, 1):
        send_sum(way, 1, way, False)
    attend(2, (1,))
    combine(3)
    attend(1, (0,))
    multiply(3)
    for way in (0, 1):
        send_sum(way, 2, 1 - way, False)
    add_on(2, (0,))
    attend(1, (1,))
    combine(2)
    attend(0)
    multiply(2)
    add_on(3, (1, 0))
    combine(1)
    combine(0)
    multiply(1)
    add_on(4, (1, 0))
    multiply(0)
    gathered(1)
    for turn in (1, 0):
        for way in (0, 1):
            sum_copy(way, 4, turn if way == 0 else 1 - turn).wait_recv()
    for h in (0, 1):
        rows = slice(16 * h, 16 * h + 16)
        for t in range(32):
            cols = slice(t * PART, (t + 1) * PART)
            mixture = part[0, rows, cols] + (
                sum_in[0, 3, h, :, cols].astype(F32) + sum_in[1, 3, h, :, cols].astype(F32)
            )
            row = 4 * (t % 2)
            gate = mod_all[1, t // 2, row : row + 1, :]
            res[rows, cols] = (lat[rows, cols].astype(F32) + gate * mixture).astype(BF16)

    store = pltpu.make_async_copy(res, result, load_sem.at[13])
    store.start()
    ring_bytes = gx.at[pl.ds(0, 7), pl.ds(0, OWN)]
    for i, ref in enumerate(
        (
            ring_bytes,
            gx.at[:, pl.ds(0, OWN)],
            mod_in.at[pl.ds(1, 15)],
            mod_all.at[0, pl.ds(0, 15)],
            mod_all.at[1, pl.ds(0, 15)],
            qs.at[pl.ds(0, 3)],
            kv.at[pl.ds(0, 3 * (ROWS + CTX))],
            outs.at[pl.ds(1, 3)],
            stats.at[:, pl.ds(1, 3)],
            att.at[:, 1],
            ring_bytes,
            wout.at[0],
        )
    ):
        arrived(ref, sent.at[i])
    store.wait()


def shards(*args):
    (
        latent,
        context,
        condition,
        context_condition,
        modulation,
        query_weight,
        key_weight,
        value_weight,
        lambdas,
        context_lift,
        head_gain,
        output_weight,
    ) = args
    anywhere = pl.BlockSpec(memory_space=pl.ANY)
    inside = pl.BlockSpec(memory_space=pltpu.VMEM)
    scalar = pl.BlockSpec(memory_space=pltpu.SMEM)
    tables = rope_tables()
    dma = pltpu.SemaphoreType.DMA
    scratch = [
        pltpu.VMEM((OWN, WIDTH), BF16),
        pltpu.VMEM((OWN, WIDTH), BF16),
        pltpu.VMEM((WIDTH // 128, 128), F32),
        pltpu.VMEM((WIDTH // 128, 128), F32),
        pltpu.VMEM((8192 // GRID_W, PART), F32),
        pltpu.VMEM((8192 // GRID_W, PART), F32),
        pltpu.VMEM((2, GRID_W, PART), F32),
        pltpu.VMEM((2, GRID_W, PART), F32),
        pltpu.VMEM((8, 64, WIDTH), BF16),
        pltpu.VMEM((CTX, WIDTH), BF16),
        pltpu.VMEM((3, 256, 256), BF16),
        pltpu.VMEM((3, WIDTH, HEAD), BF16),
        pltpu.VMEM((128, WIDTH), BF16),
        pltpu.VMEM((16, 2, 8, PART), F32),
        pltpu.VMEM((2, 16, 8, PART), F32),
        pltpu.VMEM((3, 128, HEAD), BF16),
        pltpu.VMEM((4, ROWS, HEAD), BF16),
        pltpu.VMEM((KEYS, 2 * HEAD), BF16),
        pltpu.VMEM((4, ROWS, 2 * HEAD), BF16),
        pltpu.VMEM((4, ROWS, 2 * HEAD), BF16),
        pltpu.VMEM((2, MEMBERS, 64, PART), F32),
        pltpu.VMEM((5, MEMBERS, 8, PART), F32),
        pltpu.VMEM((5, MEMBERS, 8, PART), F32),
        pltpu.VMEM((8, 2, OWN, HEAD), BF16),
        pltpu.VMEM((8, OWN, HEAD), BF16),
        pltpu.VMEM((2, HEAD, WIDTH), BF16),
        pltpu.VMEM((8, OWN, WIDTH), F32),
        pltpu.VMEM((2, 4, 2, 16, WIDTH), BF16),
        pltpu.VMEM((2, 4, 2, 16, WIDTH), BF16),
        dma((14,)),
        dma((12,)),
        dma((2, 7)),
        dma((8,)),
        dma((3,)),
        dma((9,)),
        dma((9,)),
        dma((5,)),
        dma((5,)),
        dma((5,)),
        dma(()),
        dma((2, 7)),
    ]
    return pl.pallas_call(
        body,
        out_shape=jax.ShapeDtypeStruct(latent.shape, BF16),
        in_specs=[anywhere] * 8 + [scalar, scalar, inside] + [anywhere] * 5,
        out_specs=anywhere,
        scratch_shapes=scratch,
        compiler_params=pltpu.CompilerParams(
            collective_id=0, has_side_effects=True, vmem_limit_bytes=60 * 1024 * 1024
        ),
        name="layer",
    )(
        latent,
        context,
        condition.reshape(WIDTH // 128, 128),
        context_condition.reshape(WIDTH // 128, 128),
        modulation,
        query_weight,
        key_weight,
        value_weight,
        lambdas,
        context_lift,
        head_gain.reshape(2, 128),
        output_weight,
        *tables,
    )


def solution(mesh):
    split = Mesh(mesh.devices.reshape(4, 4, 8, 2), ("y", "x", "z", "c"))
    plane = ("y", "x")
    column = ("z", "c")
    every = ("y", "x", "z", "c")
    return jax.shard_map(
        shards,
        mesh=split,
        in_specs=(
            P(every, None),
            P(plane, None),
            P(),
            P(),
            P(None, plane, column),
            P(None, column),
            P(None, column),
            P(None, column),
            P(column),
            P(column),
            P(),
            P(column, None),
        ),
        out_specs=P(every, None),
        check_vma=False,
    )
```

```python
import functools
import math

import jax
import jax.numpy as jnp
import numpy as np
from jax import lax
from jax.experimental import pallas as pl
from jax.experimental.pallas import tpu as pltpu
from jax.sharding import Mesh
from jax.sharding import PartitionSpec as P

MESH = pl.DeviceIdType.MESH
F32 = jnp.float32
BF16 = jnp.bfloat16

WIDTH = 4096
GRID_W = 64
ROPE_BASE = 10000.0
EPSILON = 1e-05
HEAD = 256
PART = 128
LOG2E = math.log2(math.e)
SCALE2 = PART ** (-0.5) * LOG2E
ROWS = 512
OWN = 32
CTX = 32
MEMBERS = 4
LAT_KEYS = MEMBERS * ROWS
KEYS = LAT_KEYS + MEMBERS * CTX
TILE = 256
OFFSET = (0, -1, 1, -2, 2, -3, 3, 4)
PASSES = ((0,), (1, 2), (3, 4), (5, 6), (7,))


def rope_tables():
    quarter = PART // 2
    eighth = PART // 4
    inverse = np.float32(ROPE_BASE) ** (-np.arange(eighth, dtype=np.float32) / np.float32(eighth))
    inverse = inverse.astype(np.float32)
    sign = np.concatenate([-np.ones(eighth), np.ones(eighth)]).astype(np.float32)

    def pair(count):
        angles = np.arange(count, dtype=np.float32)[:, None] * np.concatenate([inverse, inverse])
        angles = angles.astype(np.float32).astype(np.float64)
        return np.cos(angles).astype(np.float32), (np.sin(angles) * sign).astype(np.float32)

    row_cos, row_sin = pair(8192 // GRID_W)
    col_cos, col_sin = pair(GRID_W)
    none = np.zeros_like(row_cos)
    row_cos, row_sin = (np.concatenate([t, none], axis=1) for t in (row_cos, row_sin))
    none = np.zeros_like(col_cos)
    col_cos, col_sin = (np.concatenate([none, t], axis=1) for t in (col_cos, col_sin))
    half = GRID_W // 2
    both = [np.stack([t, np.concatenate([t[half:], t[:half]])]) for t in (col_cos, col_sin)]
    return row_cos, row_sin, both[0], both[1]


def body(
    latent,
    context,
    condition,
    context_condition,
    modulation,
    query_weight,
    key_weight,
    value_weight,
    lambdas,
    context_lift,
    head_gain,
    output_weight,
    row_cos,
    row_sin,
    col_cos,
    col_sin,
    result,
    res,
    lat,
    cond,
    cond_ctx,
    rows_cos,
    rows_sin,
    cols_cos,
    cols_sin,
    gx,
    ctx,
    modw,
    weights,
    xn,
    mod_in,
    mod_all,
    raw,
    qs,
    kv,
    outs,
    outs_in,
    score_buf,
    peak_buf,
    tab,
    stats,
    stats_in,
    att,
    att_in,
    wout,
    part,
    sum_out,
    sum_in,
    load_sem,
    sent,
    xr,
    pr,
    mr,
    qr,
    kr,
    outs_r,
    stats_r,
    att_r,
    wout_r,
    rr,
):
    y, x, z, c = (lax.axis_index(a) for a in ("y", "x", "z", "c"))
    sp = y * 4 + x
    def remote(src, dst, send, recv, to):
        return pltpu.make_async_remote_copy(
            src_ref=src, dst_ref=dst, send_sem=send, recv_sem=recv, device_id=to, device_id_type=MESH
        )

    def go(copy):
        copy.start()

    def arrived(ref, semaphore):
        pltpu.make_async_copy(ref, ref, semaphore).wait()

    partner = {"c": 1 - c}

    def on_plane(dy, dx):
        return {"y": lax.rem(y + dy, 4), "x": lax.rem(x + dx, 4)}

    def on_z(d):
        return {"z": lax.rem(z + d + 8, 8)}

    def on_queries(d):
        return {"y": lax.rem(y + d * c, 4), "x": lax.rem(x + d * (1 - c), 4)}

    def on_keys(d):
        return {"y": lax.rem(y + d * (1 - c), 4), "x": lax.rem(x + d * c, 4)}

    pairs = (
        (latent, lat),
        (condition, cond),
        (context_condition, cond_ctx),
        (modulation, modw),
        (context, ctx),
        (row_cos, rows_cos),
        (row_sin, rows_sin),
        (col_cos, cols_cos),
        (col_sin, cols_sin),
        (query_weight, weights.at[0]),
        (key_weight, weights.at[1]),
        (value_weight, weights.at[2]),
        (output_weight, wout.at[0]),
    )
    loads = [pltpu.make_async_copy(a, b, load_sem.at[i]) for i, (a, b) in enumerate(pairs)]
    for load in loads:
        load.start()

    barrier = pltpu.get_barrier_semaphore()
    plane = [(dy, dx) for dy in range(4) for dx in range(4) if dy or dx]
    plane.sort(key=lambda d: -(min(d[0], 4 - d[0]) + min(d[1], 4 - d[1])))
    column = [(dz, dc) for dz in (4, 3, 5, 2, 6, 1, 7, 0) for dc in (1, 0) if dz or dc]

    def on_column(dz, dc):
        return {"z": lax.rem(z + dz, 8), "c": 1 - c if dc else c}

    peers = [on_column(*d) for d in column] + [on_plane(*d) for d in plane]
    for peer in peers:
        pl.semaphore_signal(barrier, inc=1, device_id=peer, device_id_type=MESH)

    def centered(src, g):
        v = src[pl.ds(pl.multiple_of(g * 16, 16), 16), :].astype(F32)
        v = v - jnp.mean(v, axis=-1, keepdims=True)
        spread = jnp.mean(jnp.square(v), axis=-1, keepdims=True)
        return v * lax.rsqrt(spread + EPSILON)

    def own_group(g, carry):
        gx[0, pl.ds(pl.multiple_of(g * 16, 16), 16), :] = centered(lat, g).astype(BF16)
        return carry

    loads[0].wait()
    lax.fori_loop(0, OWN // 16, own_group, 0)
    pl.semaphore_wait(barrier, len(peers))

    def ring_slot(way, k):
        return 0 if k == 0 else 7 if k == 4 else 2 * k - 1 if way == 0 else 2 * k

    def ring_copy(way, k, h):
        rows = pl.ds(16 * h, 16)
        return remote(
            gx.at[ring_slot(way, k - 1), rows],
            gx.at[ring_slot(way, k), rows],
            sent.at[0],
            xr.at[way, 2 * (k - 1) + (h if k < 4 else 0)],
            on_z(1 if way == 0 else -1),
        )

    def across(slot, h):
        return remote(
            gx.at[slot, pl.ds(16 * h, 16)],
            gx.at[slot, pl.ds(OWN + 16 * h, 16)],
            sent.at[1],
            pr.at[slot],
            partner,
        )

    def relay(k, turn):
        for way in (0, 1):
            h = turn if way == 0 else 1 - turn
            if k == 4 and turn == 1:
                continue
            ring_copy(way, k, h).wait_recv()
            if k < 3 or (k == 3 and turn == 0):
                go(ring_copy(way, k + 1, h))
            go(across(ring_slot(way, k), h))

    for turn in (0, 1):
        for way in (0, 1):
            go(ring_copy(way, 1, turn if way == 0 else 1 - turn))
    for h in (0, 1):
        go(across(0, h))

    def silu_rows(ref):
        halves = [ref[pl.ds(2 * sp + i, 1), :] for i in (0, 1)]
        v = jnp.concatenate(halves, axis=1)
        return (v / (1.0 + jnp.exp(-v))).astype(BF16).astype(F32)

    for load in loads[1:4]:
        load.wait()
    own = silu_rows(cond)
    other = silu_rows(cond_ctx)
    at_row = lax.broadcasted_iota(jnp.int32, (16, 256), 0)
    partial = jnp.zeros((16, 256), F32)
    for r in range(3):
        lhs = jnp.where(at_row == 2 * r, own, jnp.where(at_row == 2 * r + 1, other, 0.0))
        partial += jnp.dot(lhs.astype(BF16), modw[r], preferred_element_type=F32)
    def tile_of(first):
        rows = partial[first : first + 4]
        return jnp.concatenate([rows[:, :PART], rows[:, PART:]], axis=0)

    mod_in[0, 0] = tile_of(0)
    mod_in[0, 1] = tile_of(4)

    def mod_copy(dy, dx):
        there = ((4 - dy) % 4) * 4 + (4 - dx) % 4
        return remote(
            mod_in.at[0], mod_in.at[there], sent.at[2], mr.at[0], on_plane(dy, dx)
        )

    for d in plane:
        go(mod_copy(*d))
    arrived(mod_in.at[pl.ds(1, 15)], mr.at[0])

    def total_of(which):
        lines = [
            (mod_in[4 * i, which] + mod_in[4 * i + 1, which])
            + (mod_in[4 * i + 2, which] + mod_in[4 * i + 3, which])
            for i in range(4)
        ]
        return (lines[0] + lines[1]) + (lines[2] + lines[3])

    def spread(which):
        mod_all[which, 2 * z + c] = total_of(which)
        slab = mod_all.at[which, 2 * z + c]
        for d in column:
            go(remote(slab, slab, sent.at[3 + which], mr.at[1 + which], on_column(*d)))

    def gathered(which):
        arrived(mod_all.at[which, pl.ds(0, 15)], mr.at[1 + which])

    spread(0)
    relay(1, 0)
    relay(1, 1)
    relay(2, 0)
    gathered(0)

    def shift_scale(t, which):
        tile = mod_all.at[0, t // 2]
        row = 4 * (t % 2) + which
        return tile[row : row + 1, :], 1.0 + tile[row + 2 : row + 3, :], slice(t * PART, (t + 1) * PART)

    def context_group(g, carry):
        v = centered(ctx, g)
        for t in range(32):
            offset, scaling, cols = shift_scale(t, 1)
            done = v[:, cols] * scaling + offset
            xn[pl.ds(pl.multiple_of(64 + g * 16, 16), 16), cols] = done.astype(BF16)
        return carry

    def modulated(slots):
        for t in range(32):
            offset, scaling, cols = shift_scale(t, 0)
            for i, slot in enumerate(slots):
                done = gx[slot, :, cols].astype(F32) * scaling + offset
                xn[64 * i : 64 * i + 64, cols] = done.astype(BF16)

    lane = lax.broadcasted_iota(jnp.int32, (64, PART), 1)
    low = lax.rem(lane, 64) < 32

    def project(count, first, last):
        def one(g, carry):
            raw[g, pl.ds(0, count)] = jnp.dot(
                xn[pl.ds(0, count), :], weights[g], preferred_element_type=F32
            ).astype(BF16)
            return carry

        lax.fori_loop(first, last, one, 0)

    def step(p):
        slots = PASSES[p]
        modulated(slots)
        count = 64 * len(slots)
        latent_count = count
        if p == 0:
            loads[4].wait()
            lax.fori_loop(0, CTX // 16, context_group, 0)
            count += CTX
            for load in loads[5:12]:
                load.wait()

        def turn(g):
            for i, slot in enumerate(slots):
                line = sp * 8 + lax.rem(z + OFFSET[slot] + 8, 8)
                cosine = cols_cos[c] + rows_cos[pl.ds(line, 1), :]
                sine = cols_sin[c] + rows_sin[pl.ds(line, 1), :]
                base = 64 * slot
                for m in (0, 1):
                    cols = slice(m * PART, (m + 1) * PART)
                    a = raw[g, 64 * i : 64 * i + 64, cols].astype(F32)
                    swapped = jnp.where(low, pltpu.roll(a, PART - 32, 1), pltpu.roll(a, 32, 1))
                    turned = (a * cosine + swapped * sine).astype(BF16)
                    if g == 0:
                        qs[0, base : base + 64, cols] = turned
                    else:
                        kv[base : base + 64, cols] = turned

        project(count, 1, 3)
        turn(1)
        base = 64 * slots[0]
        kv[base : base + latent_count, HEAD : 2 * HEAD] = raw[2, :latent_count, :]
        if p == 0:
            kv[LAT_KEYS : LAT_KEYS + CTX, 0:HEAD] = raw[1, 64 : 64 + CTX, :]
            kv[LAT_KEYS : LAT_KEYS + CTX, HEAD : 2 * HEAD] = raw[2, 64 : 64 + CTX, :]
        for d in near(p):
            if p == 0:
                go(context_copy(d))
            go(key_copy(p, d))
        project(latent_count, 0, 1)
        turn(0)
        for d in near(p):
            go(query_copy(p, d))

    def near(p):
        return (2, 1, 3) if p == 4 else (1, 3)

    def rows_of(p):
        return 64 * PASSES[p][0], 64 * len(PASSES[p])

    def query_copy(p, d):
        start, count = rows_of(p)
        return remote(
            qs.at[0, pl.ds(start, count)],
            qs.at[4 - d, pl.ds(start, count)],
            sent.at[5],
            qr.at[p],
            on_queries(d),
        )

    def query_relay(p, d):
        start, count = rows_of(p)
        rows = pl.ds(start + (0 if d == 1 else count // 2), count // 2)
        return remote(
            qs.at[4 - d, rows], qs.at[2, rows], sent.at[5], qr.at[5 + p], on_queries(d)
        )

    def key_copy(p, d):
        start, count = rows_of(p)
        return remote(
            kv.at[pl.ds(start, count)],
            kv.at[pl.ds((4 - d) * ROWS + start, count)],
            sent.at[6],
            kr.at[p],
            on_keys(d),
        )

    def key_relay(p, d):
        start, count = rows_of(p)
        start, count = start + (0 if d == 1 else count // 2), count // 2
        return remote(
            kv.at[pl.ds((4 - d) * ROWS + start, count)],
            kv.at[pl.ds(2 * ROWS + start, count)],
            sent.at[6],
            kr.at[5 + p],
            on_keys(d),
        )

    def context_copy(d):
        return remote(
            kv.at[pl.ds(LAT_KEYS, CTX)],
            kv.at[pl.ds(LAT_KEYS + (4 - d) * CTX, CTX)],
            sent.at[6],
            kr.at[0],
            on_keys(d),
        )

    def context_relay(d):
        skip = 0 if d == 1 else CTX // 2
        return remote(
            kv.at[pl.ds(LAT_KEYS + (4 - d) * CTX + skip, CTX // 2)],
            kv.at[pl.ds(LAT_KEYS + 2 * CTX + skip, CTX // 2)],
            sent.at[6],
            kr.at[5],
            on_keys(d),
        )

    def rows_in(p, share):
        return rows_of(p)[1] * share + (CTX * share if p == 0 else 0)

    def hand_on(p):
        arrived(kv.at[pl.ds(0, rows_in(p, 2))], kr.at[p])
        for d in (1, 3):
            if p == 0:
                go(context_relay(d))
            go(key_relay(p, d))
        arrived(qs.at[pl.ds(0, 2), pl.ds(0, rows_of(p)[1])], qr.at[p])
        for d in (1, 3):
            go(query_relay(p, d))

    def slots_in(slots):
        for slot in slots:
            arrived(gx.at[slot, pl.ds(0, OWN)], pr.at[slot])

    slots_in(PASSES[0])
    step(0)
    relay(2, 1)
    slots_in(PASSES[1])
    step(1)
    relay(3, 0)
    hand_on(0)
    slots_in(PASSES[2])
    step(2)
    relay(3, 1)
    hand_on(1)
    slots_in(PASSES[3])
    step(3)
    relay(4, 0)
    hand_on(2)
    slots_in(PASSES[4])
    step(4)
    spread(1)
    loads[12].wait()
    go(remote(wout.at[0], wout.at[1], sent.at[11], wout_r, partner))
    hand_on(3)

    for p in range(4):
        arrived(kv.at[pl.ds(0, rows_in(p, 1))], kr.at[5 + p])
        arrived(qs.at[0, pl.ds(0, rows_of(p)[1])], qr.at[5 + p])
    arrived(kv.at[pl.ds(0, rows_in(4, 3))], kr.at[4])
    arrived(qs.at[pl.ds(0, 3), pl.ds(0, rows_of(4)[1])], qr.at[4])

    lift = context_lift[0] * LOG2E
    column_of = lax.broadcasted_iota(jnp.int32, (TILE, PART), 1)

    def beside(scored, weighed):
        q = total = o = top = None
        if scored:
            slot, m = scored
            cols = slice(m * PART, (m + 1) * PART)
            q = qs[:, 64 * slot : 64 * slot + 64, cols].reshape(TILE, PART)
        if weighed:
            peak = jnp.max(peak_buf[weighed[1]], axis=1, keepdims=True)
            total = jnp.zeros((TILE, PART), F32)
            o = jnp.zeros((TILE, HEAD), F32)
        for first in range(0, KEYS, 256):
            last = min(first + 256, KEYS)
            lanes = range((last - first) // PART)
            if weighed:
                w = jnp.exp2(score_buf[weighed[1], :, first:last] - peak)
                for i in lanes:
                    total += w[:, i * PART : (i + 1) * PART]
            if scored:
                t = lax.dot_general(
                    q, kv[first:last, cols], (((1,), (1,)), ((), ())), preferred_element_type=F32
                )
                t = t * SCALE2
                if first >= LAT_KEYS:
                    t = t + lift
                score_buf[m, :, first:last] = t
                for i in lanes:
                    part_t = t[:, i * PART : (i + 1) * PART]
                    top = part_t if top is None else jnp.maximum(top, part_t)
            if weighed:
                o += jnp.dot(
                    w.astype(BF16), kv[first:last, HEAD : 2 * HEAD], preferred_element_type=F32
                )
        if scored:
            peak_buf[m] = top
        if weighed:
            slot, m = weighed
            total = jnp.sum(total, axis=1, keepdims=True)
            o = (o * (1.0 / total)).astype(BF16).reshape(MEMBERS, 64, HEAD)
            outs[:, 64 * slot : 64 * slot + 64, m * HEAD : (m + 1) * HEAD] = o
            return peak, total

    turns = (7, 5, 6, 3, 4, 1, 2, 0)

    def attend(p, parts=(0, 1)):
        first, count = rows_of(p)
        parts = [i for i in parts if i < count // 64]
        for i in parts:
            slot = first // 64 + i
            found = beside((slot, 1), (slot, 0))
            after = turns[turns.index(slot) + 1 :][:1]
            found += beside((after[0], 0) if after else None, (slot, 1))
            table = jnp.where(
                column_of == 0,
                found[0],
                jnp.where(column_of == 1, found[1], jnp.where(column_of == 2, found[2], found[3])),
            )
            tab[i] = table.reshape(MEMBERS, 64, PART)
            for j in (2, 1, 3):
                go(out_copy(p, j, slot))
        if parts[-1] < count // 64 - 1:
            return
        for j in range(MEMBERS):
            second = tab[1, j] if count > 64 else jnp.zeros((64, PART), F32)
            stats[p, j] = jnp.concatenate([tab[0, j], second], axis=0).T[:8, :]
        for j in (2, 1, 3):
            go(stats_copy(p, j))

    def out_copy(p, j, slot):
        rows = pl.ds(64 * slot, 64)
        return remote(
            outs.at[j, rows], outs_in.at[4 - j, rows], sent.at[7], outs_r.at[p], on_queries(j)
        )

    def stats_copy(p, j):
        return remote(
            stats.at[p, j], stats_in.at[p, 4 - j], sent.at[8], stats_r.at[p], on_queries(j)
        )

    def swap(p):
        slots = pl.ds(PASSES[p][0], len(PASSES[p]))
        return remote(
            att.at[slots, 1], att_in.at[slots], sent.at[9], att_r.at[p], partner
        )

    def combine(p):
        start, count = rows_of(p)
        arrived(outs_in.at[pl.ds(1, 3), pl.ds(start, count)], outs_r.at[p])
        arrived(stats_in.at[p, pl.ds(1, 3)], stats_r.at[p])
        rows = slice(start, start + count)
        tables = [stats[p, 0]] + [stats_in[p, j] for j in (1, 2, 3)]
        turned = jnp.concatenate(tables + [jnp.zeros((96, PART), F32)], axis=0).T[:count]
        means = []
        for m in (0, 1):
            peaks = [turned[:, 8 * j + 2 * m : 8 * j + 2 * m + 1] for j in range(4)]
            totals = [turned[:, 8 * j + 2 * m + 1 : 8 * j + 2 * m + 2] for j in range(4)]
            top = jnp.maximum(jnp.maximum(peaks[0], peaks[1]), jnp.maximum(peaks[2], peaks[3]))
            shares = [t * jnp.exp2(k - top) for k, t in zip(peaks, totals)]
            whole = (shares[0] + shares[1]) + (shares[2] + shares[3])
            cols = slice(m * HEAD, (m + 1) * HEAD)
            acc = outs[0, rows, cols].astype(F32) * (shares[0] / whole)
            for j in (1, 2, 3):
                acc += outs_in[j, rows, cols].astype(F32) * (shares[j] / whole)
            means.append(acc)
        difference = means[0] - lambdas[0] * means[1]
        spread = jnp.mean(jnp.square(difference), axis=1, keepdims=True)
        gain = jnp.concatenate([head_gain[0:1, :], head_gain[1:2, :]], axis=1)
        scaled = difference * lax.rsqrt(spread + EPSILON) * gain
        slot, many = PASSES[p][0], len(PASSES[p])
        att[slot : slot + many] = scaled.astype(BF16).reshape(many, 2, OWN, HEAD)
        go(swap(p))

    def multiply(p):
        swap(p).wait_recv()
        slot, many = PASSES[p][0], len(PASSES[p])
        mine = att[slot : slot + many, 0].reshape(many * OWN, HEAD)
        theirs = att_in[slot : slot + many].reshape(many * OWN, HEAD)
        for n in range(2):
            cols = slice(n * 2048, (n + 1) * 2048)
            got = jnp.dot(mine, wout[0, :, cols], preferred_element_type=F32)
            got += jnp.dot(theirs, wout[1, :, cols], preferred_element_type=F32)
            part[slot : slot + many, :, cols] = got.reshape(many, OWN, 2048)

    def sum_slot(way, t):
        return 7 if t == 1 else 2 * (5 - t) if way == 0 else 2 * (5 - t) - 1

    def sum_copy(way, t, h):
        return remote(
            sum_out.at[way, t - 1, h],
            sum_in.at[way, t - 1, h],
            sent.at[10],
            rr.at[way, 0 if t == 1 else 2 * t - 3 + h],
            on_z(1 if way == 0 else -1),
        )

    def send_sum(way, t, h, add):
        slot = sum_slot(way, t)
        for n in range(4):
            cols = slice(n * 1024, (n + 1) * 1024)
            total = part[slot, 16 * h : 16 * h + 16, cols]
            if add:
                total = total + sum_in[way, t - 2, h, :, cols].astype(F32)
            sum_out[way, t - 1, h, :, cols] = total.astype(BF16)
        go(sum_copy(way, t, h))

    def add_on(t, turns):
        for turn in turns:
            for way in (0, 1):
                h = turn if way == 0 else 1 - turn
                sum_copy(way, t - 1, h).wait_recv()
                send_sum(way, t, h, True)

    beside((turns[0], 0), None)
    attend(4)
    attend(3)
    combine(4)
    attend(2, (0,))
    remote(wout.at[0], wout.at[1], sent.at[11], wout_r, partner).wait_recv()
    multiply(4)
    for way in (0, 1):
        send_sum(way, 1, way, False)
    combine(3)
    attend(2, (1,))
    multiply(3)
    for way in (0, 1):
        send_sum(way, 2, 1 - way, False)
    add_on(2, (0,))
    attend(1)
    combine(2)
    multiply(2)
    add_on(3, (1,))
    attend(0)
    add_on(3, (0,))
    combine(1)
    multiply(1)
    add_on(4, (1,))
    combine(0)
    add_on(4, (0,))
    multiply(0)
    gathered(1)
    for turn in (1, 0):
        for way in (0, 1):
            sum_copy(way, 4, turn if way == 0 else 1 - turn).wait_recv()
    for h in (0, 1):
        rows = slice(16 * h, 16 * h + 16)
        for t in range(32):
            cols = slice(t * PART, (t + 1) * PART)
            mixture = part[0, rows, cols] + (
                sum_in[0, 3, h, :, cols].astype(F32) + sum_in[1, 3, h, :, cols].astype(F32)
            )
            row = 4 * (t % 2)
            gate = mod_all[1, t // 2, row : row + 1, :]
            res[rows, cols] = (lat[rows, cols].astype(F32) + gate * mixture).astype(BF16)

    store = pltpu.make_async_copy(res, result, load_sem.at[13])
    store.start()
    ring_bytes = gx.at[pl.ds(0, 7), pl.ds(0, OWN)]
    for i, ref in enumerate(
        (
            ring_bytes,
            gx.at[:, pl.ds(0, OWN)],
            mod_in.at[pl.ds(1, 15)],
            mod_all.at[0, pl.ds(0, 15)],
            mod_all.at[1, pl.ds(0, 15)],
            qs.at[pl.ds(0, 3)],
            kv.at[pl.ds(0, 3 * (ROWS + CTX))],
            outs.at[pl.ds(1, 3)],
            stats.at[:, pl.ds(1, 3)],
            att.at[:, 1],
            ring_bytes,
            wout.at[0],
        )
    ):
        arrived(ref, sent.at[i])
    store.wait()


def shards(*args):
    (
        latent,
        context,
        condition,
        context_condition,
        modulation,
        query_weight,
        key_weight,
        value_weight,
        lambdas,
        context_lift,
        head_gain,
        output_weight,
    ) = args
    anywhere = pl.BlockSpec(memory_space=pl.ANY)
    inside = pl.BlockSpec(memory_space=pltpu.VMEM)
    scalar = pl.BlockSpec(memory_space=pltpu.SMEM)
    tables = rope_tables()
    dma = pltpu.SemaphoreType.DMA
    scratch = [
        pltpu.VMEM((OWN, WIDTH), BF16),
        pltpu.VMEM((OWN, WIDTH), BF16),
        pltpu.VMEM((WIDTH // 128, 128), F32),
        pltpu.VMEM((WIDTH // 128, 128), F32),
        pltpu.VMEM((8192 // GRID_W, PART), F32),
        pltpu.VMEM((8192 // GRID_W, PART), F32),
        pltpu.VMEM((2, GRID_W, PART), F32),
        pltpu.VMEM((2, GRID_W, PART), F32),
        pltpu.VMEM((8, 64, WIDTH), BF16),
        pltpu.VMEM((CTX, WIDTH), BF16),
        pltpu.VMEM((3, 256, 256), BF16),
        pltpu.VMEM((3, WIDTH, HEAD), BF16),
        pltpu.VMEM((128, WIDTH), BF16),
        pltpu.VMEM((16, 2, 8, PART), F32),
        pltpu.VMEM((2, 16, 8, PART), F32),
        pltpu.VMEM((3, 128, HEAD), BF16),
        pltpu.VMEM((4, ROWS, HEAD), BF16),
        pltpu.VMEM((KEYS, 2 * HEAD), BF16),
        pltpu.VMEM((4, ROWS, 2 * HEAD), BF16),
        pltpu.VMEM((4, ROWS, 2 * HEAD), BF16),
        pltpu.VMEM((2, TILE, KEYS), F32),
        pltpu.VMEM((2, TILE, PART), F32),
        pltpu.VMEM((2, MEMBERS, 64, PART), F32),
        pltpu.VMEM((5, MEMBERS, 8, PART), F32),
        pltpu.VMEM((5, MEMBERS, 8, PART), F32),
        pltpu.VMEM((8, 2, OWN, HEAD), BF16),
        pltpu.VMEM((8, OWN, HEAD), BF16),
        pltpu.VMEM((2, HEAD, WIDTH), BF16),
        pltpu.VMEM((8, OWN, WIDTH), F32),
        pltpu.VMEM((2, 4, 2, 16, WIDTH), BF16),
        pltpu.VMEM((2, 4, 2, 16, WIDTH), BF16),
        dma((14,)),
        dma((12,)),
        dma((2, 7)),
        dma((8,)),
        dma((3,)),
        dma((9,)),
        dma((9,)),
        dma((5,)),
        dma((5,)),
        dma((5,)),
        dma(()),
        dma((2, 7)),
    ]
    return pl.pallas_call(
        body,
        out_shape=jax.ShapeDtypeStruct(latent.shape, BF16),
        in_specs=[anywhere] * 8 + [scalar, scalar, inside] + [anywhere] * 5,
        out_specs=anywhere,
        scratch_shapes=scratch,
        compiler_params=pltpu.CompilerParams(
            collective_id=0, has_side_effects=True, vmem_limit_bytes=60 * 1024 * 1024
        ),
        name="layer",
    )(
        latent,
        context,
        condition.reshape(WIDTH // 128, 128),
        context_condition.reshape(WIDTH // 128, 128),
        modulation,
        query_weight,
        key_weight,
        value_weight,
        lambdas,
        context_lift,
        head_gain.reshape(2, 128),
        output_weight,
        *tables,
    )


def solution(mesh):
    split = Mesh(mesh.devices.reshape(4, 4, 8, 2), ("y", "x", "z", "c"))
    plane = ("y", "x")
    column = ("z", "c")
    every = ("y", "x", "z", "c")
    return jax.shard_map(
        shards,
        mesh=split,
        in_specs=(
            P(every, None),
            P(plane, None),
            P(),
            P(),
            P(None, plane, column),
            P(None, column),
            P(None, column),
            P(None, column),
            P(column),
            P(column),
            P(),
            P(column, None),
        ),
        out_specs=P(every, None),
        check_vma=False,
    )
```

```python
import functools
import math

import jax
import jax.numpy as jnp
import numpy as np
from jax import lax
from jax.experimental import pallas as pl
from jax.experimental.pallas import tpu as pltpu
from jax.sharding import Mesh
from jax.sharding import PartitionSpec as P

MESH = pl.DeviceIdType.MESH
F32 = jnp.float32
BF16 = jnp.bfloat16

WIDTH = 4096
GRID_W = 64
ROPE_BASE = 10000.0
EPSILON = 1e-05
HEAD = 256
PART = 128
LOG2E = math.log2(math.e)
SCALE2 = PART ** (-0.5) * LOG2E
ROWS = 512
OWN = 32
CTX = 32
MEMBERS = 4
LAT_KEYS = MEMBERS * ROWS
KEYS = LAT_KEYS + MEMBERS * CTX
TILE = 256
OFFSET = (0, -1, 1, -2, 2, -3, 3, 4)
PASSES = ((0,), (1, 2), (3, 4), (5, 6), (7,))


def rope_tables():
    quarter = PART // 2
    eighth = PART // 4
    inverse = np.float32(ROPE_BASE) ** (-np.arange(eighth, dtype=np.float32) / np.float32(eighth))
    inverse = inverse.astype(np.float32)
    sign = np.concatenate([-np.ones(eighth), np.ones(eighth)]).astype(np.float32)

    def pair(count):
        angles = np.arange(count, dtype=np.float32)[:, None] * np.concatenate([inverse, inverse])
        angles = angles.astype(np.float32).astype(np.float64)
        return np.cos(angles).astype(np.float32), (np.sin(angles) * sign).astype(np.float32)

    row_cos, row_sin = pair(8192 // GRID_W)
    col_cos, col_sin = pair(GRID_W)
    none = np.zeros_like(row_cos)
    row_cos, row_sin = (np.concatenate([t, none], axis=1) for t in (row_cos, row_sin))
    none = np.zeros_like(col_cos)
    col_cos, col_sin = (np.concatenate([none, t], axis=1) for t in (col_cos, col_sin))
    half = GRID_W // 2
    both = [np.stack([t, np.concatenate([t[half:], t[:half]])]) for t in (col_cos, col_sin)]
    return row_cos, row_sin, both[0], both[1]


def body(
    latent,
    context,
    condition,
    context_condition,
    modulation,
    query_weight,
    key_weight,
    value_weight,
    lambdas,
    context_lift,
    head_gain,
    output_weight,
    row_cos,
    row_sin,
    col_cos,
    col_sin,
    result,
    res,
    lat,
    cond,
    cond_ctx,
    rows_cos,
    rows_sin,
    cols_cos,
    cols_sin,
    gx,
    ctx,
    modw,
    weights,
    xn,
    mod_in,
    mod_all,
    raw,
    qs,
    kv,
    outs,
    outs_in,
    score_buf,
    peak_buf,
    tab,
    stats,
    stats_in,
    att,
    att_in,
    wout,
    part,
    sum_out,
    sum_in,
    load_sem,
    sent,
    xr,
    pr,
    mr,
    qr,
    kr,
    outs_r,
    stats_r,
    att_r,
    wout_r,
    rr,
):
    y, x, z, c = (lax.axis_index(a) for a in ("y", "x", "z", "c"))
    sp = y * 4 + x
    def remote(src, dst, send, recv, to):
        return pltpu.make_async_remote_copy(
            src_ref=src, dst_ref=dst, send_sem=send, recv_sem=recv, device_id=to, device_id_type=MESH
        )

    def go(copy):
        copy.start()

    def arrived(ref, semaphore):
        pltpu.make_async_copy(ref, ref, semaphore).wait()

    partner = {"c": 1 - c}

    def on_plane(dy, dx):
        return {"y": lax.rem(y + dy, 4), "x": lax.rem(x + dx, 4)}

    def on_z(d):
        return {"z": lax.rem(z + d + 8, 8)}

    def on_queries(d):
        return {"y": lax.rem(y + d * c, 4), "x": lax.rem(x + d * (1 - c), 4)}

    def on_keys(d):
        return {"y": lax.rem(y + d * (1 - c), 4), "x": lax.rem(x + d * c, 4)}

    pairs = (
        (latent, lat),
        (condition, cond),
        (context_condition, cond_ctx),
        (modulation, modw),
        (context, ctx),
        (row_cos, rows_cos),
        (row_sin, rows_sin),
        (col_cos, cols_cos),
        (col_sin, cols_sin),
        (query_weight, weights.at[0]),
        (key_weight, weights.at[1]),
        (value_weight, weights.at[2]),
        (output_weight, wout.at[0]),
    )
    loads = [pltpu.make_async_copy(a, b, load_sem.at[i]) for i, (a, b) in enumerate(pairs)]
    for load in loads:
        load.start()

    barrier = pltpu.get_barrier_semaphore()
    plane = [(dy, dx) for dy in range(4) for dx in range(4) if dy or dx]
    plane.sort(key=lambda d: -(min(d[0], 4 - d[0]) + min(d[1], 4 - d[1])))
    column = [(dz, dc) for dz in (4, 3, 5, 2, 6, 1, 7, 0) for dc in (1, 0) if dz or dc]

    def on_column(dz, dc):
        return {"z": lax.rem(z + dz, 8), "c": 1 - c if dc else c}

    peers = [on_column(*d) for d in column] + [on_plane(*d) for d in plane]
    for peer in peers:
        pl.semaphore_signal(barrier, inc=1, device_id=peer, device_id_type=MESH)

    def centered(src, g):
        v = src[pl.ds(pl.multiple_of(g * 16, 16), 16), :].astype(F32)
        v = v - jnp.mean(v, axis=-1, keepdims=True)
        spread = jnp.mean(jnp.square(v), axis=-1, keepdims=True)
        return v * lax.rsqrt(spread + EPSILON)

    def own_group(g, carry):
        gx[0, pl.ds(pl.multiple_of(g * 16, 16), 16), :] = centered(lat, g).astype(BF16)
        return carry

    loads[0].wait()
    lax.fori_loop(0, OWN // 16, own_group, 0)
    pl.semaphore_wait(barrier, len(peers))

    def ring_slot(way, k):
        return 0 if k == 0 else 7 if k == 4 else 2 * k - 1 if way == 0 else 2 * k

    def ring_copy(way, k, h):
        rows = pl.ds(16 * h, 16)
        return remote(
            gx.at[ring_slot(way, k - 1), rows],
            gx.at[ring_slot(way, k), rows],
            sent.at[0],
            xr.at[way, 2 * (k - 1) + (h if k < 4 else 0)],
            on_z(1 if way == 0 else -1),
        )

    def across(slot, h):
        return remote(
            gx.at[slot, pl.ds(16 * h, 16)],
            gx.at[slot, pl.ds(OWN + 16 * h, 16)],
            sent.at[1],
            pr.at[slot],
            partner,
        )

    def relay(k, turn):
        for way in (0, 1):
            h = turn if way == 0 else 1 - turn
            if k == 4 and turn == 1:
                continue
            ring_copy(way, k, h).wait_recv()
            if k < 3 or (k == 3 and turn == 0):
                go(ring_copy(way, k + 1, h))
            go(across(ring_slot(way, k), h))

    for turn in (0, 1):
        for way in (0, 1):
            go(ring_copy(way, 1, turn if way == 0 else 1 - turn))
    for h in (0, 1):
        go(across(0, h))

    def silu_rows(ref):
        halves = [ref[pl.ds(2 * sp + i, 1), :] for i in (0, 1)]
        v = jnp.concatenate(halves, axis=1)
        return (v / (1.0 + jnp.exp(-v))).astype(BF16).astype(F32)

    for load in loads[1:4]:
        load.wait()
    own = silu_rows(cond)
    other = silu_rows(cond_ctx)
    at_row = lax.broadcasted_iota(jnp.int32, (16, 256), 0)
    partial = jnp.zeros((16, 256), F32)
    for r in range(3):
        lhs = jnp.where(at_row == 2 * r, own, jnp.where(at_row == 2 * r + 1, other, 0.0))
        partial += jnp.dot(lhs.astype(BF16), modw[r], preferred_element_type=F32)
    def tile_of(first):
        rows = partial[first : first + 4]
        return jnp.concatenate([rows[:, :PART], rows[:, PART:]], axis=0)

    mod_in[0, 0] = tile_of(0)
    mod_in[0, 1] = tile_of(4)

    def mod_copy(dy, dx):
        there = ((4 - dy) % 4) * 4 + (4 - dx) % 4
        return remote(
            mod_in.at[0], mod_in.at[there], sent.at[2], mr.at[0], on_plane(dy, dx)
        )

    for d in plane:
        go(mod_copy(*d))
    arrived(mod_in.at[pl.ds(1, 15)], mr.at[0])

    def total_of(which):
        lines = [
            (mod_in[4 * i, which] + mod_in[4 * i + 1, which])
            + (mod_in[4 * i + 2, which] + mod_in[4 * i + 3, which])
            for i in range(4)
        ]
        return (lines[0] + lines[1]) + (lines[2] + lines[3])

    def spread(which):
        mod_all[which, 2 * z + c] = total_of(which)
        slab = mod_all.at[which, 2 * z + c]
        for d in column:
            go(remote(slab, slab, sent.at[3 + which], mr.at[1 + which], on_column(*d)))

    def gathered(which):
        arrived(mod_all.at[which, pl.ds(0, 15)], mr.at[1 + which])

    spread(0)
    relay(1, 0)
    relay(1, 1)
    relay(2, 0)
    gathered(0)

    def shift_scale(t, which):
        tile = mod_all.at[0, t // 2]
        row = 4 * (t % 2) + which
        return tile[row : row + 1, :], 1.0 + tile[row + 2 : row + 3, :], slice(t * PART, (t + 1) * PART)

    def context_group(g, carry):
        v = centered(ctx, g)
        for t in range(32):
            offset, scaling, cols = shift_scale(t, 1)
            done = v[:, cols] * scaling + offset
            xn[pl.ds(pl.multiple_of(64 + g * 16, 16), 16), cols] = done.astype(BF16)
        return carry

    def modulated(slots):
        for t in range(32):
            offset, scaling, cols = shift_scale(t, 0)
            for i, slot in enumerate(slots):
                done = gx[slot, :, cols].astype(F32) * scaling + offset
                xn[64 * i : 64 * i + 64, cols] = done.astype(BF16)

    lane = lax.broadcasted_iota(jnp.int32, (64, PART), 1)
    low = lax.rem(lane, 64) < 32

    def project(count, first, last):
        def one(g, carry):
            raw[g, pl.ds(0, count)] = jnp.dot(
                xn[pl.ds(0, count), :], weights[g], preferred_element_type=F32
            ).astype(BF16)
            return carry

        lax.fori_loop(first, last, one, 0)

    def step(p):
        slots = PASSES[p]
        modulated(slots)
        count = 64 * len(slots)
        latent_count = count
        if p == 0:
            loads[4].wait()
            lax.fori_loop(0, CTX // 16, context_group, 0)
            count += CTX
            for load in loads[5:12]:
                load.wait()

        def turn(g):
            for i, slot in enumerate(slots):
                line = sp * 8 + lax.rem(z + OFFSET[slot] + 8, 8)
                cosine = cols_cos[c] + rows_cos[pl.ds(line, 1), :]
                sine = cols_sin[c] + rows_sin[pl.ds(line, 1), :]
                base = 64 * slot
                for m in (0, 1):
                    cols = slice(m * PART, (m + 1) * PART)
                    a = raw[g, 64 * i : 64 * i + 64, cols].astype(F32)
                    swapped = jnp.where(low, pltpu.roll(a, PART - 32, 1), pltpu.roll(a, 32, 1))
                    turned = (a * cosine + swapped * sine).astype(BF16)
                    if g == 0:
                        qs[0, base : base + 64, cols] = turned
                    else:
                        kv[base : base + 64, cols] = turned

        project(count, 1, 3)
        turn(1)
        base = 64 * slots[0]
        kv[base : base + latent_count, HEAD : 2 * HEAD] = raw[2, :latent_count, :]
        if p == 0:
            kv[LAT_KEYS : LAT_KEYS + CTX, 0:HEAD] = raw[1, 64 : 64 + CTX, :]
            kv[LAT_KEYS : LAT_KEYS + CTX, HEAD : 2 * HEAD] = raw[2, 64 : 64 + CTX, :]
        for d in near(p):
            if p == 0:
                go(context_copy(d))
            go(key_copy(p, d))
        project(latent_count, 0, 1)
        turn(0)
        for d in near(p):
            go(query_copy(p, d))

    def near(p):
        return (2, 1, 3) if p == 4 else (1, 3)

    def rows_of(p):
        return 64 * PASSES[p][0], 64 * len(PASSES[p])

    def query_copy(p, d):
        start, count = rows_of(p)
        return remote(
            qs.at[0, pl.ds(start, count)],
            qs.at[4 - d, pl.ds(start, count)],
            sent.at[5],
            qr.at[p],
            on_queries(d),
        )

    def query_relay(p, d):
        start, count = rows_of(p)
        rows = pl.ds(start + (0 if d == 1 else count // 2), count // 2)
        return remote(
            qs.at[4 - d, rows], qs.at[2, rows], sent.at[5], qr.at[5 + p], on_queries(d)
        )

    def key_copy(p, d):
        start, count = rows_of(p)
        return remote(
            kv.at[pl.ds(start, count)],
            kv.at[pl.ds((4 - d) * ROWS + start, count)],
            sent.at[6],
            kr.at[p],
            on_keys(d),
        )

    def key_relay(p, d):
        start, count = rows_of(p)
        start, count = start + (0 if d == 1 else count // 2), count // 2
        return remote(
            kv.at[pl.ds((4 - d) * ROWS + start, count)],
            kv.at[pl.ds(2 * ROWS + start, count)],
            sent.at[6],
            kr.at[5 + p],
            on_keys(d),
        )

    def context_copy(d):
        return remote(
            kv.at[pl.ds(LAT_KEYS, CTX)],
            kv.at[pl.ds(LAT_KEYS + (4 - d) * CTX, CTX)],
            sent.at[6],
            kr.at[0],
            on_keys(d),
        )

    def context_relay(d):
        skip = 0 if d == 1 else CTX // 2
        return remote(
            kv.at[pl.ds(LAT_KEYS + (4 - d) * CTX + skip, CTX // 2)],
            kv.at[pl.ds(LAT_KEYS + 2 * CTX + skip, CTX // 2)],
            sent.at[6],
            kr.at[5],
            on_keys(d),
        )

    def rows_in(p, share):
        return rows_of(p)[1] * share + (CTX * share if p == 0 else 0)

    def hand_on(p):
        arrived(kv.at[pl.ds(0, rows_in(p, 2))], kr.at[p])
        for d in (1, 3):
            if p == 0:
                go(context_relay(d))
            go(key_relay(p, d))
        arrived(qs.at[pl.ds(0, 2), pl.ds(0, rows_of(p)[1])], qr.at[p])
        for d in (1, 3):
            go(query_relay(p, d))

    def slots_in(slots):
        for slot in slots:
            arrived(gx.at[slot, pl.ds(0, OWN)], pr.at[slot])

    slots_in(PASSES[0])
    step(0)
    relay(2, 1)
    slots_in(PASSES[1])
    step(1)
    relay(3, 0)
    hand_on(0)
    slots_in(PASSES[2])
    step(2)
    relay(3, 1)
    hand_on(1)
    slots_in(PASSES[3])
    hand_on(2)
    step(3)
    relay(4, 0)
    slots_in(PASSES[4])
    step(4)
    spread(1)
    loads[12].wait()
    go(remote(wout.at[0], wout.at[1], sent.at[11], wout_r, partner))
    hand_on(3)

    for p in range(4):
        arrived(kv.at[pl.ds(0, rows_in(p, 1))], kr.at[5 + p])
        arrived(qs.at[0, pl.ds(0, rows_of(p)[1])], qr.at[5 + p])
    arrived(kv.at[pl.ds(0, rows_in(4, 3))], kr.at[4])
    arrived(qs.at[pl.ds(0, 3), pl.ds(0, rows_of(4)[1])], qr.at[4])

    lift = context_lift[0] * LOG2E
    column_of = lax.broadcasted_iota(jnp.int32, (TILE, PART), 1)

    def beside(scored, weighed):
        q = total = o = top = None
        if scored:
            slot, m = scored
            cols = slice(m * PART, (m + 1) * PART)
            q = qs[:, 64 * slot : 64 * slot + 64, cols].reshape(TILE, PART)
        if weighed:
            peak = jnp.max(peak_buf[weighed[1]], axis=1, keepdims=True)
            total = jnp.zeros((TILE, PART), F32)
            o = jnp.zeros((TILE, HEAD), F32)
        for first in range(0, KEYS, 256):
            last = min(first + 256, KEYS)
            lanes = range((last - first) // PART)
            if weighed:
                w = jnp.exp2(score_buf[weighed[1], :, first:last] - peak)
                for i in lanes:
                    total += w[:, i * PART : (i + 1) * PART]
            if scored:
                t = lax.dot_general(
                    q, kv[first:last, cols], (((1,), (1,)), ((), ())), preferred_element_type=F32
                )
                t = t * SCALE2
                if first >= LAT_KEYS:
                    t = t + lift
                score_buf[m, :, first:last] = t
                for i in lanes:
                    part_t = t[:, i * PART : (i + 1) * PART]
                    top = part_t if top is None else jnp.maximum(top, part_t)
            if weighed:
                o += jnp.dot(
                    w.astype(BF16), kv[first:last, HEAD : 2 * HEAD], preferred_element_type=F32
                )
        if scored:
            peak_buf[m] = top
        if weighed:
            slot, m = weighed
            total = jnp.sum(total, axis=1, keepdims=True)
            o = (o * (1.0 / total)).astype(BF16).reshape(MEMBERS, 64, HEAD)
            outs[:, 64 * slot : 64 * slot + 64, m * HEAD : (m + 1) * HEAD] = o
            return peak, total

    turns = (7, 5, 6, 3, 4, 1, 2, 0)

    def attend(p, parts=(0, 1)):
        first, count = rows_of(p)
        parts = [i for i in parts if i < count // 64]
        for i in parts:
            slot = first // 64 + i
            found = beside((slot, 1), (slot, 0))
            after = turns[turns.index(slot) + 1 :][:1]
            found += beside((after[0], 0) if after else None, (slot, 1))
            table = jnp.where(
                column_of == 0,
                found[0],
                jnp.where(column_of == 1, found[1], jnp.where(column_of == 2, found[2], found[3])),
            )
            tab[i] = table.reshape(MEMBERS, 64, PART)
            for j in (2, 1, 3):
                go(out_copy(p, j, slot))
        if parts[-1] < count // 64 - 1:
            return
        for j in range(MEMBERS):
            second = tab[1, j] if count > 64 else jnp.zeros((64, PART), F32)
            stats[p, j] = jnp.concatenate([tab[0, j], second], axis=0).T[:8, :]
        for j in (2, 1, 3):
            go(stats_copy(p, j))

    def out_copy(p, j, slot):
        rows = pl.ds(64 * slot, 64)
        return remote(
            outs.at[j, rows], outs_in.at[4 - j, rows], sent.at[7], outs_r.at[p], on_queries(j)
        )

    def stats_copy(p, j):
        return remote(
            stats.at[p, j], stats_in.at[p, 4 - j], sent.at[8], stats_r.at[p], on_queries(j)
        )

    def swap(p):
        slots = pl.ds(PASSES[p][0], len(PASSES[p]))
        return remote(
            att.at[slots, 1], att_in.at[slots], sent.at[9], att_r.at[p], partner
        )

    def combine(p):
        start, count = rows_of(p)
        arrived(outs_in.at[pl.ds(1, 3), pl.ds(start, count)], outs_r.at[p])
        arrived(stats_in.at[p, pl.ds(1, 3)], stats_r.at[p])
        rows = slice(start, start + count)
        tables = [stats[p, 0]] + [stats_in[p, j] for j in (1, 2, 3)]
        turned = jnp.concatenate(tables + [jnp.zeros((96, PART), F32)], axis=0).T[:count]
        means = []
        for m in (0, 1):
            peaks = [turned[:, 8 * j + 2 * m : 8 * j + 2 * m + 1] for j in range(4)]
            totals = [turned[:, 8 * j + 2 * m + 1 : 8 * j + 2 * m + 2] for j in range(4)]
            top = jnp.maximum(jnp.maximum(peaks[0], peaks[1]), jnp.maximum(peaks[2], peaks[3]))
            shares = [t * jnp.exp2(k - top) for k, t in zip(peaks, totals)]
            whole = (shares[0] + shares[1]) + (shares[2] + shares[3])
            cols = slice(m * HEAD, (m + 1) * HEAD)
            acc = outs[0, rows, cols].astype(F32) * (shares[0] / whole)
            for j in (1, 2, 3):
                acc += outs_in[j, rows, cols].astype(F32) * (shares[j] / whole)
            means.append(acc)
        difference = means[0] - lambdas[0] * means[1]
        spread = jnp.mean(jnp.square(difference), axis=1, keepdims=True)
        gain = jnp.concatenate([head_gain[0:1, :], head_gain[1:2, :]], axis=1)
        scaled = difference * lax.rsqrt(spread + EPSILON) * gain
        slot, many = PASSES[p][0], len(PASSES[p])
        att[slot : slot + many] = scaled.astype(BF16).reshape(many, 2, OWN, HEAD)
        go(swap(p))

    def multiply(p):
        swap(p).wait_recv()
        slot, many = PASSES[p][0], len(PASSES[p])
        mine = att[slot : slot + many, 0].reshape(many * OWN, HEAD)
        theirs = att_in[slot : slot + many].reshape(many * OWN, HEAD)
        for n in range(2):
            cols = slice(n * 2048, (n + 1) * 2048)
            got = jnp.dot(mine, wout[0, :, cols], preferred_element_type=F32)
            got += jnp.dot(theirs, wout[1, :, cols], preferred_element_type=F32)
            part[slot : slot + many, :, cols] = got.reshape(many, OWN, 2048)

    def sum_slot(way, t):
        return 7 if t == 1 else 2 * (5 - t) if way == 0 else 2 * (5 - t) - 1

    def sum_copy(way, t, h):
        return remote(
            sum_out.at[way, t - 1, h],
            sum_in.at[way, t - 1, h],
            sent.at[10],
            rr.at[way, 0 if t == 1 else 2 * t - 3 + h],
            on_z(1 if way == 0 else -1),
        )

    def send_sum(way, t, h, add):
        slot = sum_slot(way, t)
        for n in range(4):
            cols = slice(n * 1024, (n + 1) * 1024)
            total = part[slot, 16 * h : 16 * h + 16, cols]
            if add:
                total = total + sum_in[way, t - 2, h, :, cols].astype(F32)
            sum_out[way, t - 1, h, :, cols] = total.astype(BF16)
        go(sum_copy(way, t, h))

    def add_on(t, turns):
        for turn in turns:
            for way in (0, 1):
                h = turn if way == 0 else 1 - turn
                sum_copy(way, t - 1, h).wait_recv()
                send_sum(way, t, h, True)

    beside((turns[0], 0), None)
    attend(4)
    attend(3)
    combine(4)
    attend(2, (0,))
    remote(wout.at[0], wout.at[1], sent.at[11], wout_r, partner).wait_recv()
    multiply(4)
    for way in (0, 1):
        send_sum(way, 1, way, False)
    combine(3)
    attend(2, (1,))
    multiply(3)
    for way in (0, 1):
        send_sum(way, 2, 1 - way, False)
    add_on(2, (0,))
    attend(1)
    combine(2)
    multiply(2)
    add_on(3, (1,))
    attend(0)
    add_on(3, (0,))
    combine(1)
    multiply(1)
    add_on(4, (1,))
    combine(0)
    add_on(4, (0,))
    multiply(0)
    gathered(1)
    for turn in (1, 0):
        for way in (0, 1):
            sum_copy(way, 4, turn if way == 0 else 1 - turn).wait_recv()
    for h in (0, 1):
        rows = slice(16 * h, 16 * h + 16)
        for t in range(32):
            cols = slice(t * PART, (t + 1) * PART)
            mixture = part[0, rows, cols] + (
                sum_in[0, 3, h, :, cols].astype(F32) + sum_in[1, 3, h, :, cols].astype(F32)
            )
            row = 4 * (t % 2)
            gate = mod_all[1, t // 2, row : row + 1, :]
            res[rows, cols] = (lat[rows, cols].astype(F32) + gate * mixture).astype(BF16)

    store = pltpu.make_async_copy(res, result, load_sem.at[13])
    store.start()
    ring_bytes = gx.at[pl.ds(0, 7), pl.ds(0, OWN)]
    for i, ref in enumerate(
        (
            ring_bytes,
            gx.at[:, pl.ds(0, OWN)],
            mod_in.at[pl.ds(1, 15)],
            mod_all.at[0, pl.ds(0, 15)],
            mod_all.at[1, pl.ds(0, 15)],
            qs.at[pl.ds(0, 3)],
            kv.at[pl.ds(0, 3 * (ROWS + CTX))],
            outs.at[pl.ds(1, 3)],
            stats.at[:, pl.ds(1, 3)],
            att.at[:, 1],
            ring_bytes,
            wout.at[0],
        )
    ):
        arrived(ref, sent.at[i])
    store.wait()


def shards(*args):
    (
        latent,
        context,
        condition,
        context_condition,
        modulation,
        query_weight,
        key_weight,
        value_weight,
        lambdas,
        context_lift,
        head_gain,
        output_weight,
    ) = args
    anywhere = pl.BlockSpec(memory_space=pl.ANY)
    inside = pl.BlockSpec(memory_space=pltpu.VMEM)
    scalar = pl.BlockSpec(memory_space=pltpu.SMEM)
    tables = rope_tables()
    dma = pltpu.SemaphoreType.DMA
    scratch = [
        pltpu.VMEM((OWN, WIDTH), BF16),
        pltpu.VMEM((OWN, WIDTH), BF16),
        pltpu.VMEM((WIDTH // 128, 128), F32),
        pltpu.VMEM((WIDTH // 128, 128), F32),
        pltpu.VMEM((8192 // GRID_W, PART), F32),
        pltpu.VMEM((8192 // GRID_W, PART), F32),
        pltpu.VMEM((2, GRID_W, PART), F32),
        pltpu.VMEM((2, GRID_W, PART), F32),
        pltpu.VMEM((8, 64, WIDTH), BF16),
        pltpu.VMEM((CTX, WIDTH), BF16),
        pltpu.VMEM((3, 256, 256), BF16),
        pltpu.VMEM((3, WIDTH, HEAD), BF16),
        pltpu.VMEM((128, WIDTH), BF16),
        pltpu.VMEM((16, 2, 8, PART), F32),
        pltpu.VMEM((2, 16, 8, PART), F32),
        pltpu.VMEM((3, 128, HEAD), BF16),
        pltpu.VMEM((4, ROWS, HEAD), BF16),
        pltpu.VMEM((KEYS, 2 * HEAD), BF16),
        pltpu.VMEM((4, ROWS, 2 * HEAD), BF16),
        pltpu.VMEM((4, ROWS, 2 * HEAD), BF16),
        pltpu.VMEM((2, TILE, KEYS), F32),
        pltpu.VMEM((2, TILE, PART), F32),
        pltpu.VMEM((2, MEMBERS, 64, PART), F32),
        pltpu.VMEM((5, MEMBERS, 8, PART), F32),
        pltpu.VMEM((5, MEMBERS, 8, PART), F32),
        pltpu.VMEM((8, 2, OWN, HEAD), BF16),
        pltpu.VMEM((8, OWN, HEAD), BF16),
        pltpu.VMEM((2, HEAD, WIDTH), BF16),
        pltpu.VMEM((8, OWN, WIDTH), F32),
        pltpu.VMEM((2, 4, 2, 16, WIDTH), BF16),
        pltpu.VMEM((2, 4, 2, 16, WIDTH), BF16),
        dma((14,)),
        dma((12,)),
        dma((2, 7)),
        dma((8,)),
        dma((3,)),
        dma((9,)),
        dma((9,)),
        dma((5,)),
        dma((5,)),
        dma((5,)),
        dma(()),
        dma((2, 7)),
    ]
    return pl.pallas_call(
        body,
        out_shape=jax.ShapeDtypeStruct(latent.shape, BF16),
        in_specs=[anywhere] * 8 + [scalar, scalar, inside] + [anywhere] * 5,
        out_specs=anywhere,
        scratch_shapes=scratch,
        compiler_params=pltpu.CompilerParams(
            collective_id=0, has_side_effects=True, vmem_limit_bytes=60 * 1024 * 1024
        ),
        name="layer",
    )(
        latent,
        context,
        condition.reshape(WIDTH // 128, 128),
        context_condition.reshape(WIDTH // 128, 128),
        modulation,
        query_weight,
        key_weight,
        value_weight,
        lambdas,
        context_lift,
        head_gain.reshape(2, 128),
        output_weight,
        *tables,
    )


def solution(mesh):
    split = Mesh(mesh.devices.reshape(4, 4, 8, 2), ("y", "x", "z", "c"))
    plane = ("y", "x")
    column = ("z", "c")
    every = ("y", "x", "z", "c")
    return jax.shard_map(
        shards,
        mesh=split,
        in_specs=(
            P(every, None),
            P(plane, None),
            P(),
            P(),
            P(None, plane, column),
            P(None, column),
            P(None, column),
            P(None, column),
            P(column),
            P(column),
            P(),
            P(column, None),
        ),
        out_specs=P(every, None),
        check_vma=False,
    )
```
